512 devices in a mesh: rep: 2 (over z_hi), fs: 32 (over z_lo, y), tp: 8 (over x, core).
Axes of the slice: x: 4, y: 4, z: 16 (z_hi: 2, z_lo: 8; z = z_hi * 8 + z_lo), core: 2. Of those that a mesh axis runs over, the one named last changes fastest.
Arguments:
- tokens: bfloat16 [16384, 2048], P(('rep', 'fs')), may hold values from -6 to 6
- ffn_gate: bfloat16 [2048, 5632], P('fs', 'tp'), may hold values from -0.125 to 0.125
- ffn_up: bfloat16 [2048, 5632], P('fs', 'tp'), may hold values from -0.125 to 0.125
- ffn_down: bfloat16 [5632, 2048], P('tp', 'fs'), may hold values from -0.3125 to 0.3125
- query_proj: bfloat16 [2048, 512], P('fs', 'tp'), may hold values from -0.125 to 0.125
- key_proj: bfloat16 [2048, 512], P('fs', 'tp'), may hold values from -0.125 to 0.125
- value_proj: bfloat16 [2048, 1024], P('fs', 'tp'), may hold values from -0.125 to 0.125
- outgate_proj: bfloat16 [2048, 1024], P('fs', 'tp'), may hold values from -0.125 to 0.125
- output_proj: bfloat16 [1024, 2048], P('tp', 'fs'), may hold values from -0.375 to 0.375
- rank_down: bfloat16 [2048, 16], replicated, may hold values from -0.1875 to 0.1875
- rank_up: bfloat16 [16, 512], replicated, may hold values from -3 to 3
- decay_bias: float32 [512], replicated, may hold values from -0.5 to 8
- head_gain: float32 [1024], replicated, may hold values from 0.1 to 1.9
- norm_gain: float32 [3, 2048], replicated, may hold values from 0.1 to 1.9
- norm_bias: float32 [3, 2048], replicated, may hold values from -2 to 2
Outputs:
- layer_out: bfloat16 [16384, 2048], P(('rep', 'fs'))
The draws below stay inside these ranges and needn't reach their ends.
All inputs are finite; a program needn't handle non-finite values.
Results may differ from the reference program's by a relative error of at most 0.024.
Values may be sent and summed in bfloat16 or wider, within the bound.
A program may use at most 64 MiB of HBM per device.

```python
import jax
import jax.numpy as jnp
from jax import lax

D = 2048
FF = 5632
HEADS = 8
DK = 64
DV = 128
RANK = 16
BLOCK = 64
TOK = 256
TOKENS = 16384
N_TP = 8


def draw_decay_bias(key, part):
    pick_key, slow_key, fast_key, jitter_key = jax.random.split(jax.random.fold_in(key, 11), 4)
    chance = 0.5
    slow_heads = jax.random.uniform(pick_key, (HEADS, 1), jnp.float32) < chance
    slow_level = jax.random.uniform(slow_key, (HEADS, 1), jnp.float32, 5.5, 7.5)
    fast_level = jax.random.uniform(fast_key, (HEADS, 1), jnp.float32, 0.0, 1.5)
    jitter = jax.random.uniform(jitter_key, (HEADS, DK), jnp.float32, -0.5, 0.5)
    return (jnp.where(slow_heads, slow_level, fast_level) + jitter).reshape(HEADS * DK).astype(jnp.float32)


def level_of(own_key, extent, shards, least, largest):
    factor_of, own = 1.0, jax.random.fold_in(own_key, 6)
    for axis_at, shards_of in shards:
        heights = jnp.exp(jax.random.uniform(jax.random.fold_in(own, axis_at), (shards_of,), jnp.float32, least / len(shards), largest / len(shards)))
        factor_of = factor_of * jnp.repeat(heights, extent[axis_at] // shards_of).reshape([-1 if axis == axis_at else 1 for axis in range(len(extent))])
    return factor_of


def bell_draw(key, extent, scale, bound, cuts=(), dtype=jnp.bfloat16):
    result = jax.random.normal(key, extent, jnp.float32) * scale
    if len(cuts) > 0:
        result = level_of(key, extent, cuts, -0.22, 0.18) * result
    return jnp.clip(result, min=-bound, max=bound).astype(dtype)


def setup_inputs(seed: int = 0) -> dict:
    splits = jax.random.split(jax.random.key(seed), 16)
    return {
        "tokens": bell_draw(splits[0], (TOKENS, D), 1.0, 6.0, ((0, 64),)),
        "ffn_gate": bell_draw(splits[1], (D, FF), D ** -0.5, 0.125, ((0, 32), (1, 8))),
        "ffn_up": bell_draw(splits[2], (D, FF), D ** -0.5, 0.125, ((0, 32), (1, 8))),
        "ffn_down": bell_draw(splits[3], (FF, D), (FF // 16) ** -0.5, 0.3125, ((0, 8), (1, 32))),
        "query_proj": bell_draw(splits[4], (D, HEADS * DK), D ** -0.5, 0.125, ((0, 32), (1, 8))),
        "key_proj": bell_draw(splits[5], (D, HEADS * DK), D ** -0.5, 0.125, ((0, 32), (1, 8))),
        "value_proj": bell_draw(splits[6], (D, HEADS * DV), D ** -0.5, 0.125, ((0, 32), (1, 8))),
        "outgate_proj": bell_draw(splits[7], (D, HEADS * DV), D ** -0.5, 0.125, ((0, 32), (1, 8))),
        "output_proj": bell_draw(splits[8], (HEADS * DV, D), (HEADS * DV // 4) ** -0.5, 0.375, ((0, 8), (1, 32))),
        "rank_down": bell_draw(splits[9], (D, RANK), (D // 2) ** -0.5, 0.1875),
        "rank_up": bell_draw(splits[10], (RANK, HEADS * DK), (RANK // 4) ** -0.5, 3.0),
        "decay_bias": draw_decay_bias(jax.random.fold_in(splits[15], 71), 0),
        "head_gain": jnp.clip(1.0 + 0.18 * jax.random.normal(splits[12], (HEADS * DV,), jnp.float32), 0.1, 1.9),
        "norm_gain": jnp.clip(1.0 + 0.18 * jax.random.normal(splits[13], (3, D), jnp.float32), 0.1, 1.9),
        "norm_bias": bell_draw(splits[14], (3, D), 0.3, 2.0, (), jnp.float32),
    }


EPSILON = 1e-05
HEAD_FLOOR = 1.0
RESIDUAL_SCALE = 2.0 ** 0.5
GATE_SOFTNESS = 16.0
FULL_ACCURACY = lax.Precision.HIGHEST

def layer_norm(summed, norm_gain, norm_shift):
    centred = summed - lax.optimization_barrier(jnp.mean(summed, -1, keepdims=True))
    spread = lax.optimization_barrier(jnp.mean(centred * centred, -1, keepdims=True))
    return (centred * lax.rsqrt(spread + EPSILON) * norm_gain + norm_shift).astype(jnp.bfloat16)

def gla_heads(queries, keys_rows, values, decay_logarithm):
    length, head_count, key_width = queries.shape
    value_width = values.shape[-1]
    block_count = length // BLOCK

    def blocks(array):
        return array.reshape(block_count, BLOCK, head_count, array.shape[-1])
    causal = jnp.tril(jnp.ones((BLOCK, BLOCK), bool))[:, :, None, None]

    def advance(running_state, inputs):
        query_block, key_block, value_block, decay_blk = inputs
        decay_prefix = jnp.cumsum(decay_blk, axis=0)
        spread = decay_prefix[:, None] - decay_prefix[None, :]
        weight = jnp.exp(jnp.where(causal, spread, -jnp.inf))
        scores = jnp.einsum('lshk,lhk,shk->hls', weight, query_block, key_block, precision=FULL_ACCURACY)
        within = jnp.einsum('hls,shv->lhv', scores, value_block, precision=FULL_ACCURACY)
        carried_over = jnp.einsum('zew,ewa->zea', query_block * jnp.exp(decay_prefix), running_state, precision=FULL_ACCURACY)
        block_finish = decay_prefix[-1]
        running_state = jnp.exp(block_finish)[:, :, None] * running_state + jnp.einsum('oct,ocy->cty', key_block * jnp.exp(block_finish[None] - decay_prefix), value_block, precision=FULL_ACCURACY)
        return (running_state, within + carried_over)
    initial = jnp.zeros((head_count, key_width, value_width), jnp.float32)
    _, outputs = lax.scan(advance, initial, (blocks(queries), blocks(keys_rows), blocks(values), blocks(decay_logarithm)))
    return outputs.reshape(length, head_count, value_width)

def block_partials(hidden, weight):
    width = weight.shape[0] // N_TP
    summed = jnp.zeros((hidden.shape[0], weight.shape[1]), jnp.float32)
    for block in range(N_TP):
        product = jnp.dot(hidden[:, block * width:(block + 1) * width], weight[block * width:(block + 1) * width], preferred_element_type=jnp.float32)
        rounded = lax.optimization_barrier(product.astype(jnp.bfloat16))
        summed = summed + rounded.astype(jnp.float32)
    return summed

def reference(tokens, ffn_gate, ffn_up, ffn_down, query_proj, key_proj, value_proj, outgate_proj, output_proj, rank_down, rank_up, decay_bias, head_gain, norm_gain, norm_bias):

    def channel_mix(normed):
        gate_rows = jnp.dot(normed, ffn_gate, preferred_element_type=jnp.float32)
        up_rows = jnp.dot(normed, ffn_up, preferred_element_type=jnp.float32)
        hidden = (jax.nn.silu(gate_rows) * up_rows).astype(jnp.bfloat16)
        return block_partials(hidden, ffn_down)

    def one_sequence(rows):
        first = layer_norm(RESIDUAL_SCALE * rows.astype(jnp.float32) + 0.5 * channel_mix(rows), norm_gain[0], norm_bias[0])
        queries = jnp.dot(first, query_proj, preferred_element_type=jnp.float32) * DK ** (-0.5)
        keys_rows = jnp.dot(first, key_proj, preferred_element_type=jnp.float32)
        values = jnp.dot(first, value_proj, preferred_element_type=jnp.float32)
        gates = jnp.dot(first, outgate_proj, preferred_element_type=jnp.float32)
        rank_rows = jnp.dot(first, rank_down, preferred_element_type=jnp.float32)
        decay_source = jnp.dot(rank_rows, rank_up.astype(jnp.float32), precision=FULL_ACCURACY) + decay_bias
        decay_logarithm = jax.nn.log_sigmoid(decay_source) / GATE_SOFTNESS
        length = rows.shape[0]
        heads_out = gla_heads(queries.reshape(length, HEADS, DK), keys_rows.reshape(length, HEADS, DK), values.reshape(length, HEADS, DV), decay_logarithm.reshape(length, HEADS, DK))
        scaled = heads_out * lax.rsqrt(lax.optimization_barrier(jnp.mean(heads_out * heads_out, -1, keepdims=True)) + HEAD_FLOOR)
        scaled = scaled * head_gain.reshape(HEADS, DV)
        mixed = (scaled.reshape(length, HEADS * DV) * jax.nn.silu(gates)).astype(jnp.bfloat16)
        second = layer_norm(RESIDUAL_SCALE * first.astype(jnp.float32) + block_partials(mixed, output_proj), norm_gain[1], norm_bias[1])
        return layer_norm(RESIDUAL_SCALE * second.astype(jnp.float32) + 0.5 * channel_mix(second), norm_gain[2], norm_bias[2])
    sequences = tokens.reshape(TOKENS // TOK, TOK, D)
    return lax.map(one_sequence, sequences).reshape(TOKENS, D)
```

```python
import functools
import heapq

import jax
import jax.numpy as jnp
from jax import lax
from jax.experimental import pallas as pl
from jax.experimental.pallas import tpu as pltpu
from jax.sharding import Mesh
from jax.sharding import PartitionSpec as P

DK = 64
DV = 128
FS = ("fs_0", "fs_1")
REP_FS = ("rep", "fs_0", "fs_1")
NZ, NY, NX = 8, 4, 4
ROWS = 256
D = 2048
SHARD = 64
COLS = 256
OWN = 32

EPSILON = 1e-05
HEAD_FLOOR = 1.0
RESIDUAL_SCALE = 2.0**0.5
GATE_SOFTNESS = 16.0

MESH = pl.DeviceIdType.MESH
F32 = jnp.float32
BF16 = jnp.bfloat16
LINKS = ("z+", "z-", "y+", "y-")
WIDTHS = ((7, 4), (3, 3), (2, 2))
NEAREST = (0, 1, -1, 2, -2, 3, -3, 4)


def gather_items():
    items = []

    def add(chunk, part, link, slot, half, depth):
        dz, dy = slot
        lands = {"z+": (dz - 1, dy), "z-": (dz + 1, dy), "y+": (dz, dy - 1), "y-": (dz, dy + 1)}[link]
        size = WIDTHS[chunk][part] * (1.0 if half is None else 0.5)
        items.append((chunk, part, link, slot, half, lands, depth, size))

    def along_z(chunk, part, dy, more):
        for s in range(4):
            add(chunk, part, "z+", (-s, dy), None if s < 3 else 0, 4 - s + more)
            add(chunk, part, "z-", (s, dy), None if s < 3 else 1, 4 - s + more)

    def along_y(chunk, part, dz, more):
        add(chunk, part, "y+", (dz, 0), None, 2 + more)
        add(chunk, part, "y-", (dz, 0), None, 2 + more)
        add(chunk, part, "y+", (dz, -1), 0, 1 + more)
        add(chunk, part, "y-", (dz, 1), 1, 1 + more)

    for chunk in range(len(WIDTHS)):
        along_z(chunk, 0, 0, 2)
        for dz in NEAREST:
            along_y(chunk, 0, dz, 0)
        along_y(chunk, 1, 0, 4)
        for dy in (0, 1, -1, 2):
            along_z(chunk, 1, dy, 0)
    return items


def spot(slot):
    return (slot[0] % NZ, slot[1] % NY)


def gather_order(backlog=2.0, tile_us=0.352, fixed=0.05, hop=2.2):
    items = gather_items()
    held = {(c, p, (0, 0)): {0, 1} for c in range(len(WIDTHS)) for p in (0, 1)}
    waiting = list(range(len(items)))
    ready = {link: [] for link in LINKS}
    free = {link: 0.0 for link in LINKS}
    order, flying = [], []

    def step(now):
        left = []
        for i in waiting:
            chunk, part, link, slot, half = items[i][:5]
            have = held.get((chunk, part, spot(slot)), set())
            if have >= ({0, 1} if half is None else {half}):
                ready[link].append(i)
            else:
                left.append(i)
        waiting[:] = left
        for link in LINKS:
            ready[link].sort(key=lambda i: (items[i][0], -items[i][6], i))
            while ready[link] and free[link] - now < backlog:
                i = ready[link].pop(0)
                free[link] = max(now, free[link]) + items[i][7] * tile_us + fixed
                heapq.heappush(flying, (free[link] + hop, i))
                order.append((now, "send", i))

    step(0.0)
    while flying:
        now, i = heapq.heappop(flying)
        chunk, part, _, _, half, lands = items[i][:6]
        held.setdefault((chunk, part, spot(lands)), set()).update({0, 1} if half is None else {half})
        order.append((now, "land", i))
        step(now)
    return items, order


def dot_nt(a, b):
    return lax.dot_general(a, b, (((1,), (1,)), ((), ())), preferred_element_type=F32)


def dot_nn(a, b, precision=None):
    return lax.dot_general(a, b, (((1,), (0,)), ((), ())), preferred_element_type=F32, precision=precision)


def silu(v):
    return v / (1.0 + jnp.exp(-v))


def boundary(prefix, m):
    if m >= 4:
        parts = prefix.reshape(ROWS // (2 * m), 2 * m, DK)
        edge = jnp.broadcast_to(parts[:, m - 1 : m, :], parts.shape)
        return edge.reshape(ROWS, DK)
    parts = prefix.reshape(ROWS // 8, 8, DK)
    row = lax.broadcasted_iota(jnp.int32, parts.shape, 1)
    edge = jnp.broadcast_to(parts[:, 8 - m - 1 : 8 - m, :], parts.shape)
    for at in range(8 - 4 * m, -1, -2 * m):
        edge = jnp.where(row < at + 2 * m, jnp.broadcast_to(parts[:, at + m - 1 : at + m, :], parts.shape), edge)
    return edge.reshape(ROWS, DK)


def head_out(q, k, v, log_decay):
    row = lax.broadcasted_iota(jnp.int32, (ROWS, ROWS), 0)
    col = lax.broadcasted_iota(jnp.int32, (ROWS, ROWS), 1)
    prefix = dot_nn((col <= row).astype(F32), log_decay, lax.Precision.HIGHEST)
    apart = row ^ col
    scores = jnp.where(row == col, jnp.sum(q * k, axis=1, keepdims=True), 0.0)
    m = ROWS // 2
    while m:
        fade = jnp.exp(-jnp.abs(prefix - boundary(prefix, m)))
        level = dot_nt((q * fade).astype(BF16), (k * fade).astype(BF16))
        scores = jnp.where((row > col) & (apart >= m) & (apart < 2 * m), level, scores)
        m //= 2
    return dot_nn(scores.astype(BF16), v.astype(BF16))


def layer_kernel(items, order, *refs):
    (tok, ga, gb, da, db, qa, qb, rank_down, rank_up, bias, head_gain, norm_gain, norm_bias) = refs[:13]
    out = refs[13]
    (GA, GB, DA, DB, QA, QB, acc_a, acc_b, hid, first, second, mixed, sendbuf, pairbuf, xsend, xrecv, tot) = refs[14:31]
    (put_sem, get_sem, own_sem, pair_s, pair_r, x_s, x_r, ag_s, ag_r) = refs[31:]
    shards = ((ga, gb), (da, db), (qa, qb))
    bufs = ((GA, GB), (DA, DB), (QA, QB))

    rep, zl, y, tp = (lax.axis_index(a) for a in ("rep", "fs_0", "fs_1", "tp"))
    zg = rep * NZ + zl
    x, c = tp // 2, lax.rem(tp, 2)
    other = 1 - c

    def at_z(step):
        g = lax.rem(zg + step + 16, 16)
        return (g // NZ, lax.rem(g, NZ), y, tp)

    def at_y(step):
        return (rep, zl, lax.rem(y + step + NY, NY), tp)

    def at_x(step):
        return (rep, zl, y, lax.rem(x + step + NX, NX) * 2 + c)

    partner = (rep, zl, y, x * 2 + other)
    where = {"z+": at_z(1), "z-": at_z(-1), "y+": at_y(1), "y-": at_y(-1)}
    xs = [at_x(s) for s in (1, 2, 3)]
    from_x = [lax.rem(x - s + NX, NX) for s in (1, 2, 3)]
    z_at = {k: lax.rem(zl + k, NZ) for k in range(NZ)}
    y_at = {k: lax.rem(y + k, NY) for k in range(NY)}

    barrier = pltpu.get_barrier_semaphore()
    friends = list(where.values()) + xs + [partner]
    for friend in friends:
        pl.semaphore_signal(barrier, inc=1, device_id=friend, device_id_type=MESH)
    owns = []
    for k in range(3):
        for p in range(2):
            copy = pltpu.make_async_copy(shards[k][p], bufs[k][p].at[zl, y], own_sem.at[2 * k + p])
            copy.start()
            owns.append(copy)
    pl.semaphore_wait(barrier, len(friends))

    def place(chunk, part, slot, half):
        dz, dy = spot(slot)
        buf = bufs[chunk][part]
        if half is None:
            return buf.at[z_at[dz], y_at[dy]]
        return buf.at[z_at[dz], y_at[dy], pl.ds(32 * half, 32)]

    def item_copy(i, landing):
        chunk, part, link, slot, half, lands = items[i][:6]
        here = place(chunk, part, lands if landing else slot, half)
        src = here
        if not landing and spot(slot) == (0, 0):
            src = shards[chunk][part] if half is None else shards[chunk][part].at[pl.ds(32 * half, 32)]
        return pltpu.make_async_remote_copy(
            src_ref=src, dst_ref=here, send_sem=put_sem.at[i], recv_sem=get_sem.at[i],
            device_id=where[link], device_id_type=MESH)

    def near(i):
        return lax.rem(zl + ((i + 1) // 2) * (2 * lax.rem(i, 2) - 1) + NZ, NZ)

    def gate_up(source, lo, hi):
        def step(i, carry):
            zi = near(i)
            a = source[:, pl.ds(pl.multiple_of(zi * COLS, COLS), COLS)]
            acc_a[...] += dot_nn(a, GA[zi].reshape(COLS, 896))
            acc_b[...] += dot_nn(a, GB[zi].reshape(COLS, 512))
            return carry
        lax.fori_loop(lo, hi, step, 0)

    def clear():
        acc_a[...] = jnp.zeros_like(acc_a)
        acc_b[...] = jnp.zeros_like(acc_b)

    def hidden():
        hid[:, 0:256] = (silu(acc_a[:, 0:256]) * acc_a[:, 640:896]).astype(BF16)
        hid[:, 256:640] = (silu(acc_a[:, 256:640]) * acc_b[:, 0:384]).astype(BF16)
        last = acc_b[:, 384:512]
        lane = lax.broadcasted_iota(jnp.int32, last.shape, 1)
        mixed_last = silu(last) * pltpu.roll(last, 64, 1)
        hid[:, 640:768] = jnp.where(lane < 64, mixed_last, 0.0).astype(BF16)

    def down_part(zi):
        return dot_nt(hid[:, :384], DA[zi].reshape(COLS, 384)) + dot_nt(hid[:, 384:], DB[zi].reshape(COLS, 384))

    def output_part(zi):
        return dot_nt(mixed[...], QB[zi][:, :, 128:].reshape(COLS, 128))

    def pair_copy(zi):
        return pltpu.make_async_remote_copy(
            src_ref=sendbuf.at[zi, other], dst_ref=pairbuf.at[zi], send_sem=pair_s.at[zi], recv_sem=pair_r.at[zi],
            device_id=partner, device_id_type=MESH)

    def x_copy(zi, s):
        return pltpu.make_async_remote_copy(
            src_ref=xsend.at[zi, lax.rem(x + s + 1, NX)], dst_ref=xrecv.at[s, zi],
            send_sem=x_s.at[s, zi], recv_sem=x_r.at[s, zi], device_id=xs[s], device_id_type=MESH)

    def front(part, zi):
        value = part(zi)
        for t in range(8):
            sendbuf[zi, t % 2, t // 2] = value[t * OWN : (t + 1) * OWN].astype(BF16)
        pair_copy(zi).start()

    def middle(zi):
        pair_copy(zi).wait_recv()
        xsend[zi] = (sendbuf[zi, c].astype(F32) + pairbuf[zi].astype(F32)).astype(BF16)
        for s in (1, 0, 2):
            x_copy(zi, s).start()

    row0 = pl.multiple_of(tp * OWN, OWN)

    def settle(source, target, factor, which):
        def wait(zi, carry):
            for s in range(3):
                x_copy(zi, s).wait_recv()
            return carry
        lax.fori_loop(0, NZ, wait, 0)
        own = source[pl.ds(row0, OWN), :].astype(F32)
        total = jnp.zeros((OWN, 1), F32)
        for zi in range(NZ):
            part = sendbuf[zi, c, x].astype(F32) + pairbuf[zi, x].astype(F32)
            for s in range(3):
                part = part + xrecv[s, zi].astype(F32)
            part = RESIDUAL_SCALE * own[:, zi * COLS : (zi + 1) * COLS] + factor * part
            tot[:, zi * COLS : (zi + 1) * COLS] = part
            total = total + jnp.sum(part, axis=1, keepdims=True)
        centred = tot[...] - total * (1.0 / D)
        spread = jnp.mean(centred * centred, axis=1, keepdims=True)
        normed = centred * lax.rsqrt(spread + EPSILON) * norm_gain[which : which + 1, :] + norm_bias[which : which + 1, :]
        target[pl.ds(row0, OWN), :] = normed.astype(BF16)

    def rows_of(target, xx, cc, half):
        start = pl.multiple_of((xx * 2 + cc) * OWN + 16 * half, 16)
        return target.at[pl.ds(start, 16)]

    def ag_copy(target, k, half, xx, cc, to):
        ref = rows_of(target, xx, cc, half)
        return pltpu.make_async_remote_copy(
            src_ref=ref, dst_ref=ref, send_sem=ag_s.at[k, half], recv_sem=ag_r.at[k, half],
            device_id=to, device_id_type=MESH)

    def spread_out(target):
        for half in range(2):
            for s in (1, 0, 2):
                ag_copy(target, s, half, x, c, xs[s]).start()
        for half in range(2):
            ag_copy(target, 3, half, x, c, partner).start()

    def pass_on(target, s, half):
        ag_copy(target, s, half, from_x[s], c, xs[s]).wait_recv()
        ag_copy(target, 4 + s, half, from_x[s], c, partner).start()

    def gathered(target):
        for half in range(2):
            ag_copy(target, 3, half, x, other, partner).wait_recv()
        for half in range(2):
            for s in range(3):
                ag_copy(target, 4 + s, half, from_x[s], other, partner).wait_recv()

    def drain(target):
        def wait(zi, carry):
            pair_copy(zi).wait_send()
            for s in range(3):
                x_copy(zi, s).wait_send()
            return carry
        lax.fori_loop(0, NZ, wait, 0)
        for half in range(2):
            for s in range(3):
                ag_copy(target, s, half, x, c, xs[s]).wait_send()
                ag_copy(target, 4 + s, half, from_x[s], c, partner).wait_send()
            ag_copy(target, 3, half, x, c, partner).wait_send()

    held = {}
    done_groups = [[], [], []]
    state = {"gate": 0, "fronts": [], "middles": []}
    end_of = [max(t for t, kind, i in order if kind == "land" and items[i][0] == k) for k in range(3)]
    steps = [(t, 0, kind, i) for t, kind, i in order]
    steps += [(end_of[1] + 4.5, 1, "settle", 0)]
    steps += [(end_of[1] + 4.6, 2, "spread", 0)]
    at = end_of[1] + 8.0
    for half in range(2):
        for s in (0, 2, 1):
            steps.append((at + 1.5 * half + (0.7 if s == 1 else 0.0), 3, "pass", (s, half)))
    steps.sort(key=lambda e: e[:2])
    clear()

    def flush_middles(keep):
        while len(state["middles"]) > keep:
            middle(state["middles"].pop(0))

    for now, _, kind, what in steps:
        if kind == "send":
            item_copy(what, False).start()
        elif kind == "land":
            item_copy(what, True).wait_recv()
            chunk, part, _, _, half, lands = items[what][:6]
            key = (chunk, spot(lands)[0])
            held[key] = held.get(key, 0.0) + (1.0 if half is None else 0.5)
            full = 6.0 if spot(lands)[0] == 0 else 8.0
            if held[key] == full:
                done_groups[chunk].append(spot(lands)[0])
                if chunk == 0 and spot(lands)[0] == 0:
                    for copy in owns:
                        copy.wait()
            if chunk == 0 and {spot((k, 0))[0] for k in NEAREST[:5]} <= set(done_groups[0]) and state["gate"] == 0:
                gate_up(tok, 0, 5)
                state["gate"] = 5
            if chunk == 0 and len(done_groups[0]) == NZ and state["gate"] == 5:
                gate_up(tok, 5, 8)
                hidden()
                state["gate"] = 8
            if state["gate"] == 8:
                for k in done_groups[1]:
                    if k not in state["fronts"]:
                        state["fronts"].append(k)
                        front(down_part, z_at[k])
                        state["middles"].append(z_at[k])
                        flush_middles(2)
                if len(state["fronts"]) == NZ:
                    flush_middles(0)
        elif kind == "settle":
            settle(tok, first, 0.5, 0)
        elif kind == "spread":
            spread_out(first)
        else:
            pass_on(first, *what)
    gathered(first)

    rows = first[...]
    proj = dot_nn(rows, QA[...].reshape(D, 256))
    gates = dot_nn(rows, QB[:, :, :, :128].reshape(D, 128))
    ranks = dot_nt(rows, rank_down[...])
    source = dot_nn(ranks, rank_up[...], lax.Precision.HIGHEST) + bias[...]
    log_decay = (jnp.minimum(source, 0.0) - jnp.log1p(jnp.exp(-jnp.abs(source)))) * (1.0 / GATE_SOFTNESS)
    heads = head_out(proj[:, :DK] * DK**-0.5, proj[:, DK : 2 * DK], proj[:, 2 * DK :], log_decay)
    scale = lax.rsqrt(jnp.mean(heads * heads, axis=1, keepdims=True) + HEAD_FLOOR)
    mixed[...] = (heads * scale * head_gain[...] * silu(gates)).astype(BF16)
    drain(first)

    def reduce_scatter(part, lag):
        def fronts(zi, carry):
            front(part, zi)
            return carry

        def both(zi, carry):
            front(part, zi)
            middle(zi - lag)
            return carry

        def middles(zi, carry):
            middle(zi)
            return carry
        lax.fori_loop(0, lag, fronts, 0)
        lax.fori_loop(lag, NZ, both, 0)
        lax.fori_loop(NZ - lag, NZ, middles, 0)

    def all_rows(target):
        spread_out(target)
        for half in range(2):
            for s in (0, 2, 1):
                pass_on(target, s, half)
        gathered(target)

    reduce_scatter(output_part, 3)
    settle(first, second, 1.0, 1)
    all_rows(second)

    clear()
    gate_up(second, 0, 8)
    hidden()
    drain(second)
    reduce_scatter(down_part, 3)
    settle(second, out, 0.5, 2)
    all_rows(out)
    drain(out)

    for t, kind, i in order:
        if kind == "send":
            item_copy(i, False).wait_send()


def per_device(
    tokens, ffn_gate, ffn_up, ffn_down, query_proj, key_proj, value_proj, outgate_proj, output_proj,
    rank_down, rank_up, decay_bias, head_gain, norm_gain, norm_bias,
):
    tp = lax.axis_index("tp")
    ga = jnp.concatenate([ffn_gate[:, :640], ffn_up[:, :256]], axis=1)
    gb = jnp.concatenate([ffn_up[:, 256:640], ffn_gate[:, 640:], ffn_up[:, 640:]], axis=1)
    down = jnp.pad(ffn_down.T, ((0, 0), (0, 64)))
    da, db = down[:, :384], down[:, 384:]
    qa = jnp.concatenate([query_proj, key_proj, value_proj], axis=1)
    qb = jnp.concatenate([outgate_proj, output_proj.T], axis=1)
    up_block = lax.dynamic_slice_in_dim(rank_up, tp * DK, DK, 1).astype(F32)
    bias_block = lax.dynamic_slice_in_dim(decay_bias, tp * DK, DK, 0).reshape(1, DK)
    gain_block = lax.dynamic_slice_in_dim(head_gain, tp * DV, DV, 0).reshape(1, DV)
    items, order = gather_order()
    count = len(items)
    dma = pltpu.SemaphoreType.DMA
    vmem = pl.BlockSpec(memory_space=pltpu.VMEM)
    scratch = [
        pltpu.VMEM((NZ, NY, SHARD, 896), BF16),
        pltpu.VMEM((NZ, NY, SHARD, 512), BF16),
        pltpu.VMEM((NZ, NY, SHARD, 384), BF16),
        pltpu.VMEM((NZ, NY, SHARD, 384), BF16),
        pltpu.VMEM((NZ, NY, SHARD, 256), BF16),
        pltpu.VMEM((NZ, NY, SHARD, 256), BF16),
        pltpu.VMEM((ROWS, 896), F32),
        pltpu.VMEM((ROWS, 512), F32),
        pltpu.VMEM((ROWS, 768), BF16),
        pltpu.VMEM((ROWS, D), BF16),
        pltpu.VMEM((ROWS, D), BF16),
        pltpu.VMEM((ROWS, DV), BF16),
        pltpu.VMEM((NZ, 2, NX, OWN, COLS), BF16),
        pltpu.VMEM((NZ, NX, OWN, COLS), BF16),
        pltpu.VMEM((NZ, NX, OWN, COLS), BF16),
        pltpu.VMEM((3, NZ, OWN, COLS), BF16),
        pltpu.VMEM((OWN, D), F32),
        dma((count,)), dma((count,)), dma((6,)),
        dma((NZ,)), dma((NZ,)), dma((3, NZ)), dma((3, NZ)), dma((7, 2)), dma((7, 2)),
    ]
    return pl.pallas_call(
        functools.partial(layer_kernel, items, order),
        out_shape=jax.ShapeDtypeStruct((ROWS, D), BF16),
        in_specs=[vmem] * 13,
        out_specs=vmem,
        scratch_shapes=scratch,
        compiler_params=pltpu.CompilerParams(
            collective_id=0, has_side_effects=True, vmem_limit_bytes=60 * 1024 * 1024),
        name="layer",
    )(tokens, ga, gb, da, db, qa, qb, rank_down.T, up_block, bias_block, gain_block, norm_gain, norm_bias)


def solution(mesh):
    finer = Mesh(
        mesh.devices.reshape(mesh.shape["rep"], NZ, NY, mesh.shape["tp"]),
        ("rep", "fs_0", "fs_1", "tp"),
    )
    return jax.shard_map(
        per_device,
        mesh=finer,
        in_specs=(
            P(REP_FS, None), P(FS, "tp"), P(FS, "tp"), P("tp", FS), P(FS, "tp"), P(FS, "tp"), P(FS, "tp"),
            P(FS, "tp"), P("tp", FS), P(), P(), P(), P(), P(), P(),
        ),
        out_specs=P(REP_FS, None),
        check_vma=False,
    )
```

```python
import functools
import heapq

import jax
import jax.numpy as jnp
from jax import lax
from jax.experimental import pallas as pl
from jax.experimental.pallas import tpu as pltpu
from jax.sharding import Mesh
from jax.sharding import PartitionSpec as P

DK = 64
DV = 128
FS = ("fs_0", "fs_1")
REP_FS = ("rep", "fs_0", "fs_1")
NZ, NY, NX = 8, 4, 4
ROWS = 256
D = 2048
SHARD = 64
COLS = 256
OWN = 32
LANES = 128

EPSILON = 1e-05
HEAD_FLOOR = 1.0
RESIDUAL_SCALE = 2.0**0.5
GATE_SOFTNESS = 16.0

MESH = pl.DeviceIdType.MESH
F32 = jnp.float32
BF16 = jnp.bfloat16
LINKS = ("z+", "z-", "y+", "y-")
WIDTHS = ((7, 4), (3, 3), (3, 1))
NEAREST = (0, 1, -1, 2, -2, 3, -3, 4)
CHUNK_LATE = (0.0, 3.33, 13.5)
FIRST_Z = (5.8, 6.9, 4.1, 3.2)
THEN_Y = (6.4, 0.0)
FIRST_Y = (8.4, 6.6)
THEN_Z = ((2.7, 6.6, 1.6, -2.6), (3.9, 1.4, 1.8, -1.1), (4.2, 1.6, 5.2, 1.5))
BACKLOG = 2.525


def gather_items():
    items = []

    def add(chunk, part, link, slot, half, rise):
        dz, dy = slot
        lands = {"z+": (dz - 1, dy), "z-": (dz + 1, dy), "y+": (dz, dy - 1), "y-": (dz, dy + 1)}[link]
        size = WIDTHS[chunk][part] * (1.0 if half is None else 0.5)
        items.append((chunk, part, link, slot, half, lands, CHUNK_LATE[chunk] - rise, size))

    def along_z(chunk, part, dy, rise):
        for s in range(4):
            add(chunk, part, "z+", (-s, dy), None if s < 3 else 0, rise[s])
            add(chunk, part, "z-", (s, dy), None if s < 3 else 1, rise[s])

    def along_y(chunk, part, dz, rise):
        add(chunk, part, "y+", (dz, 0), None, rise[0])
        add(chunk, part, "y-", (dz, 0), None, rise[0])
        add(chunk, part, "y+", (dz, -1), 0, rise[1])
        add(chunk, part, "y-", (dz, 1), 1, rise[1])

    for chunk in range(len(WIDTHS)):
        along_z(chunk, 0, 0, FIRST_Z)
        for dz in NEAREST:
            along_y(chunk, 0, dz, THEN_Y)
        along_y(chunk, 1, 0, FIRST_Y)
        for dy in (0, 1, -1, 2):
            along_z(chunk, 1, dy, THEN_Z[abs(dy)])
    return items


def spot(slot):
    return (slot[0] % NZ, slot[1] % NY)


def gather_order(backlog=BACKLOG, tile_us=0.352, fixed=0.05, hop=2.2):
    items = gather_items()
    held = {(c, p, (0, 0)): {0, 1} for c in range(len(WIDTHS)) for p in (0, 1)}
    waiting = list(range(len(items)))
    ready = {link: [] for link in LINKS}
    free = {link: 0.0 for link in LINKS}
    order, flying = [], []

    def step(now):
        left = []
        for i in waiting:
            chunk, part, link, slot, half = items[i][:5]
            have = held.get((chunk, part, spot(slot)), set())
            if have >= ({0, 1} if half is None else {half}):
                ready[link].append(i)
            else:
                left.append(i)
        waiting[:] = left
        for link in LINKS:
            ready[link].sort(key=lambda i: (items[i][6], i))
            while ready[link] and free[link] - now < backlog:
                i = ready[link].pop(0)
                free[link] = max(now, free[link]) + items[i][7] * tile_us + fixed
                heapq.heappush(flying, (free[link] + hop, i))
                order.append((now, "send", i))

    step(0.0)
    while flying:
        now, i = heapq.heappop(flying)
        chunk, part, _, _, half, lands = items[i][:6]
        held.setdefault((chunk, part, spot(lands)), set()).update({0, 1} if half is None else {half})
        order.append((now, "land", i))
        step(now)
    return items, order


def dot_nt(a, b):
    return lax.dot_general(a, b, (((1,), (1,)), ((), ())), preferred_element_type=F32)


def dot_nn(a, b, precision=None):
    return lax.dot_general(a, b, (((1,), (0,)), ((), ())), preferred_element_type=F32, precision=precision)


def silu(v):
    return v / (1.0 + jnp.exp(-v))


def boundary(prefix, m):
    if m >= 4:
        parts = prefix.reshape(ROWS // (2 * m), 2 * m, DK)
        edge = jnp.broadcast_to(parts[:, m - 1 : m, :], parts.shape)
        return edge.reshape(ROWS, DK)
    parts = prefix.reshape(ROWS // 8, 8, DK)
    row = lax.broadcasted_iota(jnp.int32, parts.shape, 1)
    edge = jnp.broadcast_to(parts[:, 8 - m - 1 : 8 - m, :], parts.shape)
    for at in range(8 - 4 * m, -1, -2 * m):
        edge = jnp.where(row < at + 2 * m, jnp.broadcast_to(parts[:, at + m - 1 : at + m, :], parts.shape), edge)
    return edge.reshape(ROWS, DK)


def head_out(q, k, v, log_decay):
    row = lax.broadcasted_iota(jnp.int32, (ROWS, ROWS), 0)
    col = lax.broadcasted_iota(jnp.int32, (ROWS, ROWS), 1)
    prefix = dot_nn((col <= row).astype(F32), log_decay, lax.Precision.HIGHEST)
    apart = row ^ col
    scores = jnp.where(row == col, jnp.sum(q * k, axis=1, keepdims=True), 0.0)
    m = ROWS // 2
    while m:
        fade = jnp.exp(-jnp.abs(prefix - boundary(prefix, m)))
        level = dot_nt((q * fade).astype(BF16), (k * fade).astype(BF16))
        scores = jnp.where((row > col) & (apart >= m) & (apart < 2 * m), level, scores)
        m //= 2
    return dot_nn(scores.astype(BF16), v.astype(BF16))


def layer_kernel(items, order, *refs):
    sources = refs[:15]
    out = refs[15]
    staged = refs[16:31]
    (tok, gate, up, down, query, key, value, outgate, output, rank_down, rank_up, bias, head_gain, norm_gain,
     norm_bias) = staged
    (GA, GB, DA, DB, QA, QB, acc, hid, first, second, third, mixed, sendbuf, pairbuf, xsend, xrecv, tot) = refs[31:48]
    (put_sem, get_sem, own_sem, pair_s, pair_r, x_s, x_r, ag_s, ag_r, out_sem) = refs[48:]
    bufs = ((GA, GB), (DA, DB), (QA, QB))
    cuts = [a * LANES for a, _ in WIDTHS]

    rep, zl, y, tp = (lax.axis_index(a) for a in ("rep", "fs_0", "fs_1", "tp"))
    zg = rep * NZ + zl
    x, c = tp // 2, lax.rem(tp, 2)
    other = 1 - c

    def at_z(step):
        g = lax.rem(zg + step + 16, 16)
        return (g // NZ, lax.rem(g, NZ), y, tp)

    def at_y(step):
        return (rep, zl, lax.rem(y + step + NY, NY), tp)

    def at_x(step):
        return (rep, zl, y, lax.rem(x + step + NX, NX) * 2 + c)

    partner = (rep, zl, y, x * 2 + other)
    where = {"z+": at_z(1), "z-": at_z(-1), "y+": at_y(1), "y-": at_y(-1)}
    xs = [at_x(s) for s in (1, 2, 3)]
    from_x = [lax.rem(x - s + NX, NX) for s in (1, 2, 3)]
    z_at = {k: lax.rem(zl + k, NZ) for k in range(NZ)}
    y_at = {k: lax.rem(y + k, NY) for k in range(NY)}

    barrier = pltpu.get_barrier_semaphore()
    friends = list(where.values()) + xs + [partner]
    for friend in friends:
        pl.semaphore_signal(barrier, inc=1, device_id=friend, device_id_type=MESH)
    loads = [pltpu.make_async_copy(a, b, own_sem.at[k]) for k, (a, b) in enumerate(zip(sources, staged))]
    for k in (1, 2, 3, 4, 5, 6, 7, 8, 0, 9, 10, 11, 12, 13, 14):
        loads[k].start()

    def pack(pair, cut, at, piece):
        stop = at + piece.shape[1]
        if at < cut:
            pair[0][zl, y, :, at : min(stop, cut)] = piece[:, : min(stop, cut) - at]
        if stop > cut:
            lo = max(at, cut)
            pair[1][zl, y, :, lo - cut : stop - cut] = piece[:, lo - at :]

    def side_by_side(a, b):
        return jnp.concatenate([a.astype(F32), b.astype(F32)], axis=1).astype(BF16)

    with jax.named_scope("pack"):
        for k in range(1, 9):
            loads[k].wait()
        pack(bufs[0], cuts[0], 0, gate[:, 0:640])
        pack(bufs[0], cuts[0], 640, up[:, 0:640])
        pack(bufs[0], cuts[0], 1280, side_by_side(gate[:, 640:704], up[:, 640:704]))
        pack(bufs[1], cuts[1], 0, down[:, 0:640])
        pack(bufs[1], cuts[1], 640, side_by_side(down[:, 640:704], jnp.zeros((SHARD, 64), BF16)))
        pack(bufs[2], cuts[2], 0, side_by_side(query[...], key[...]))
        pack(bufs[2], cuts[2], 128, value[...])
        pack(bufs[2], cuts[2], 256, outgate[...])
        pack(bufs[2], cuts[2], 384, output[...])
    with jax.named_scope("barrier"):
        pl.semaphore_wait(barrier, len(friends))

    def place(chunk, part, slot, half):
        dz, dy = spot(slot)
        buf = bufs[chunk][part]
        if half is None:
            return buf.at[z_at[dz], y_at[dy]]
        return buf.at[z_at[dz], y_at[dy], pl.ds(32 * half, 32)]

    def item_copy(i, landing):
        chunk, part, link, slot, half, lands = items[i][:6]
        here = place(chunk, part, lands if landing else slot, half)
        return pltpu.make_async_remote_copy(
            src_ref=here, dst_ref=here, send_sem=put_sem.at[i], recv_sem=get_sem.at[i],
            device_id=where[link], device_id_type=MESH)

    def near(i):
        return lax.rem(zl + ((i + 1) // 2) * (2 * lax.rem(i, 2) - 1) + NZ, NZ)

    def gate_up(source, rows, lo, hi):
        def step(i, carry):
            zi = near(i)
            a = source[:, pl.ds(pl.multiple_of(zi * COLS, COLS), COLS)]
            acc[rows, : cuts[0]] += dot_nn(a, GA[zi].reshape(COLS, cuts[0]))
            acc[rows, cuts[0] :] += dot_nn(a, GB[zi].reshape(COLS, 1408 - cuts[0]))
            return carry
        lax.fori_loop(lo, hi, step, 0)

    def clear(rows):
        acc[rows, :] = jnp.zeros((rows.stop - rows.start, 1408), F32)

    def hidden(rows):
        hid[rows, 0:640] = (silu(acc[rows, 0:640]) * acc[rows, 640:1280]).astype(BF16)
        last = acc[rows, 1280:1408]
        lane = lax.broadcasted_iota(jnp.int32, last.shape, 1)
        mixed_last = silu(last) * pltpu.roll(last, 64, 1)
        hid[rows, 640:768] = jnp.where(lane < 64, mixed_last, 0.0).astype(BF16)

    def down_part(rows):
        def part(zi):
            cut = cuts[1]
            return dot_nt(hid[rows, :cut], DA[zi].reshape(COLS, cut)) + dot_nt(
                hid[rows, cut:], DB[zi].reshape(COLS, 768 - cut))
        return part

    def pair_copy(zi, half):
        if half is None:
            src, dst, sem = sendbuf.at[zi, other], pairbuf.at[zi], 0
        else:
            rows, both = pl.ds(16 * half, 16), pl.ds(zi, 2)
            src, dst, sem = sendbuf.at[both, other, :, rows], pairbuf.at[both, :, rows], half
        return pltpu.make_async_remote_copy(
            src_ref=src, dst_ref=dst, send_sem=pair_s.at[sem, zi], recv_sem=pair_r.at[sem, zi],
            device_id=partner, device_id_type=MESH)

    def x_copy(zi, s, half):
        to = lax.rem(x + s + 1, NX)
        if half is None:
            src, dst, sem = xsend.at[zi, to], xrecv.at[s, zi], 0
        else:
            rows, both = pl.ds(16 * half, 16), pl.ds(zi, 2)
            src, dst, sem = xsend.at[both, to, rows], xrecv.at[s, both, rows], half
        return pltpu.make_async_remote_copy(
            src_ref=src, dst_ref=dst, send_sem=x_s.at[sem, s, zi], recv_sem=x_r.at[sem, s, zi],
            device_id=xs[s], device_id_type=MESH)

    def middle(zi, half):
        pair_copy(zi, half).wait_recv()
        if half is None:
            xsend[zi] = (sendbuf[zi, c].astype(F32) + pairbuf[zi].astype(F32)).astype(BF16)
        else:
            rows = slice(16 * half, 16 * half + 16)
            for k in range(2):
                xsend[zi + k, :, rows] = (
                    sendbuf[zi + k, c, :, rows].astype(F32) + pairbuf[zi + k, :, rows].astype(F32)
                ).astype(BF16)
        for s in (1, 0, 2):
            x_copy(zi, s, half).start()

    def settle(residual, store, factor, which, half):
        rows = slice(0, OWN) if half is None else slice(16 * half, 16 * half + 16)
        if half is None:
            def wait(zi, carry):
                for s in range(3):
                    x_copy(zi, s, None).wait_recv()
                return carry
            lax.fori_loop(0, NZ, wait, 0)
        else:
            def wait(k, carry):
                for s in range(3):
                    x_copy(2 * k, s, half).wait_recv()
                return carry
            lax.fori_loop(0, NZ // 2, wait, 0)
        own = residual.astype(F32)
        total = 0.0
        for zi in range(NZ):
            part = sendbuf[zi, c, x, rows].astype(F32) + pairbuf[zi, x, rows].astype(F32)
            for s in range(3):
                part = part + xrecv[s, zi, rows].astype(F32)
            part = RESIDUAL_SCALE * own[:, zi * COLS : (zi + 1) * COLS] + factor * part
            tot[rows, zi * COLS : (zi + 1) * COLS] = part
            total = total + jnp.sum(part, axis=1, keepdims=True)
        centred = tot[rows, :] - total * (1.0 / D)
        spread = jnp.mean(centred * centred, axis=1, keepdims=True)
        normed = centred * lax.rsqrt(spread + EPSILON) * norm_gain[which : which + 1, :] + norm_bias[which : which + 1, :]
        store(normed.astype(BF16))

    def block(target, xx, cc, half):
        t = xx * 2 + cc
        if target is second:
            return target.at[half, pl.ds(pl.multiple_of(t * 16, 16), 16)]
        return target.at[pl.ds(pl.multiple_of(t * OWN + 16 * half, 16), 16)]

    def ag_copy(target, k, half, xx, cc, to):
        ref = block(target, xx, cc, half)
        return pltpu.make_async_remote_copy(
            src_ref=ref, dst_ref=ref, send_sem=ag_s.at[k, half], recv_sem=ag_r.at[k, half],
            device_id=to, device_id_type=MESH)

    def spread_out(target, half):
        for s in (1, 0, 2):
            ag_copy(target, s, half, x, c, xs[s]).start()
        ag_copy(target, 3, half, x, c, partner).start()

    def pass_on(target, s, half):
        ag_copy(target, s, half, from_x[s], c, xs[s]).wait_recv()
        ag_copy(target, 4 + s, half, from_x[s], c, partner).start()

    def pass_all(target, half):
        for s in (0, 2, 1):
            pass_on(target, s, half)

    def gathered(target, half):
        ag_copy(target, 3, half, x, other, partner).wait_recv()
        for s in range(3):
            ag_copy(target, 4 + s, half, from_x[s], other, partner).wait_recv()

    def drain_rows(target, half):
        for s in range(3):
            ag_copy(target, s, half, x, c, xs[s]).wait_send()
            ag_copy(target, 4 + s, half, from_x[s], c, partner).wait_send()
        ag_copy(target, 3, half, x, c, partner).wait_send()

    def drain_sums(half):
        stride = 1 if half is None else 2

        def wait(k, carry):
            pair_copy(k * stride, half).wait_send()
            for s in range(3):
                x_copy(k * stride, s, half).wait_send()
            return carry
        lax.fori_loop(0, NZ // stride, wait, 0)

    every = slice(0, ROWS)
    row0 = pl.multiple_of(tp * OWN, OWN)
    held = {}
    done_groups = [[], [], []]
    state = {"gate": 0, "fronts": [], "middles": []}
    end_of = [max(t for t, kind, i in order if kind == "land" and items[i][0] == k) for k in range(3)]
    steps = [(t, 0, kind, i) for t, kind, i in order]
    steps += [(end_of[1] + 4.5, 1, "settle", 0)]
    at = end_of[1] + 8.0
    for half in range(2):
        for s in (0, 2, 1):
            steps.append((at + 1.5 * half + (0.7 if s == 1 else 0.0), 3, "pass", (s, half)))
    steps.sort(key=lambda e: e[:2])
    clear(every)
    loads[0].wait()
    for k in range(9, 15):
        loads[k].wait()

    def first_front(zi):
        value = down_part(every)(zi)
        for t in range(8):
            sendbuf[zi, t % 2, t // 2] = value[t * OWN : (t + 1) * OWN].astype(BF16)
        pair_copy(zi, None).start()

    def flush_middles(keep):
        while len(state["middles"]) > keep:
            with jax.named_scope("mid1"):
                middle(state["middles"].pop(0), None)

    for now, _, kind, what in steps:
        if kind == "send":
            item_copy(what, False).start()
        elif kind == "land":
            chunk, part, _, _, half, lands = items[what][:6]
            with jax.named_scope("land%d" % chunk):
                item_copy(what, True).wait_recv()
            key_ = (chunk, spot(lands)[0])
            held[key_] = held.get(key_, 0.0) + (1.0 if half is None else 0.5)
            full = 6.0 if spot(lands)[0] == 0 else 8.0
            if held[key_] == full:
                done_groups[chunk].append(spot(lands)[0])
            if chunk == 0 and {spot((k, 0))[0] for k in NEAREST[:5]} <= set(done_groups[0]) and state["gate"] == 0:
                with jax.named_scope("gu_a"):
                    gate_up(tok, every, 0, 5)
                state["gate"] = 5
            if chunk == 0 and len(done_groups[0]) == NZ and state["gate"] == 5:
                with jax.named_scope("gu_b"):
                    gate_up(tok, every, 5, 8)
                    hidden(every)
                state["gate"] = 8
            if state["gate"] == 8:
                for k in done_groups[1]:
                    if k not in state["fronts"]:
                        state["fronts"].append(k)
                        with jax.named_scope("front1"):
                            first_front(z_at[k])
                        state["middles"].append(z_at[k])
                        flush_middles(2)
                if len(state["fronts"]) == NZ:
                    flush_middles(0)
        elif kind == "settle":
            def store_first(normed):
                first[pl.ds(row0, OWN), :] = normed
            with jax.named_scope("settle1"):
                settle(tok[pl.ds(row0, OWN), :], store_first, 0.5, 0, None)
            spread_out(first, 0)
            spread_out(first, 1)
        else:
            with jax.named_scope("pass1"):
                pass_on(first, *what)
    with jax.named_scope("gathered1"):
        gathered(first, 0)
        gathered(first, 1)

    with jax.named_scope("proj"):
        rows = first[...]
        pieces = [dot_nn(rows, QA[...].reshape(D, cuts[2]))]
        if cuts[2] < 384:
            pieces.append(dot_nn(rows, QB[:, :, :, : 384 - cuts[2]].reshape(D, 384 - cuts[2])))
        proj = jnp.concatenate(pieces, axis=1)
        ranks = dot_nt(rows, rank_down[...])
        pair_at = pl.multiple_of(x * 128, 128)

        def mine(ref):
            both = ref[:, pl.ds(pair_at, 128)].astype(F32)
            return jnp.where(c == 0, both[:, :64], both[:, 64:])
        source = dot_nn(ranks, mine(rank_up), lax.Precision.HIGHEST) + mine(bias)
        log_decay = (jnp.minimum(source, 0.0) - jnp.log1p(jnp.exp(-jnp.abs(source)))) * (1.0 / GATE_SOFTNESS)
    with jax.named_scope("gla"):
        heads = head_out(proj[:, :DK] * DK**-0.5, proj[:, DK : 2 * DK], proj[:, 128:256], log_decay)
        scale = lax.rsqrt(jnp.mean(heads * heads, axis=1, keepdims=True) + HEAD_FLOOR)
        gain = head_gain[:, pl.ds(pl.multiple_of(tp * DV, DV), DV)]
        mixed[...] = (heads * scale * gain * silu(proj[:, 256:384])).astype(BF16)
    drain_sums(None)

    def output_fronts(k):
        part = dot_nt(mixed[...], QB[4 * k : 4 * k + 4, :, :, -128:].reshape(4 * COLS, 128))
        for g in range(4):
            for t in range(8):
                sendbuf[4 * k + g, t % 2, t // 2] = part[
                    t * OWN : (t + 1) * OWN, g * COLS : (g + 1) * COLS].astype(BF16)
        for half in range(2):
            for g in range(0, 4, 2):
                pair_copy(4 * k + g, half).start()

    def middles(half, lo, hi):
        def step(k, carry):
            middle(2 * k, half)
            return carry
        lax.fori_loop(lo, hi, step, 0)

    with jax.named_scope("rs2"):
        output_fronts(0)
        output_fronts(1)
        middles(0, 0, 4)
        middles(1, 0, 4)

    leaving = []

    def put_out(k, half, xx, cc):
        copy = pltpu.make_async_copy(block(third, xx, cc, half), block(out, xx, cc, half), out_sem.at[k, half])
        copy.start()
        leaving.append(copy)

    def settle_second(half):
        def store(normed):
            second[half, pl.ds(pl.multiple_of(tp * 16, 16), 16), :] = normed
        start = pl.multiple_of(row0 + 16 * half, 16)
        settle(first[pl.ds(start, 16), :], store, 1.0, 1, half)
        spread_out(second, half)

    def settle_last(half):
        def store(normed):
            third[pl.ds(pl.multiple_of(row0 + 16 * half, 16), 16), :] = normed
        settle(second[half, pl.ds(pl.multiple_of(tp * 16, 16), 16), :], store, 0.5, 2, half)
        spread_out(third, half)
        put_out(7, half, x, c)

    def rows_of(half):
        return slice(128 * half, 128 * half + 128)

    def mixer_front(half):
        rows = rows_of(half)
        acc[rows, : cuts[0]] = dot_nn(second[half], GA[...].reshape(D, cuts[0]))
        acc[rows, cuts[0] :] = dot_nn(second[half], GB[...].reshape(D, 1408 - cuts[0]))
        hidden(rows)

    def down_sums(half):
        rows, cut = rows_of(half), cuts[1]
        for k in range(2):
            groups = slice(4 * k, 4 * k + 4)
            part = dot_nt(hid[rows, :cut], DA[groups].reshape(4 * COLS, cut)) + dot_nt(
                hid[rows, cut:], DB[groups].reshape(4 * COLS, 768 - cut))
            for g in range(4):
                for t in range(8):
                    sendbuf[4 * k + g, t % 2, t // 2, 16 * half : 16 * half + 16] = part[
                        t * 16 : (t + 1) * 16, g * COLS : (g + 1) * COLS].astype(BF16)
            for g in range(0, 4, 2):
                pair_copy(4 * k + g, half).start()
        middles(half, 0, 4)

    with jax.named_scope("settle2a"):
        settle_second(0)
    with jax.named_scope("settle2b"):
        settle_second(1)
    with jax.named_scope("pass2a"):
        pass_all(second, 0)
        gathered(second, 0)
    with jax.named_scope("gu2a"):
        mixer_front(0)
    with jax.named_scope("pass2b"):
        pass_all(second, 1)
    with jax.named_scope("rs3a"):
        drain_sums(0)
        down_sums(0)
    with jax.named_scope("gathered2b"):
        gathered(second, 1)
    with jax.named_scope("gu2b"):
        mixer_front(1)
    with jax.named_scope("rs3b"):
        drain_sums(1)
        down_sums(1)
    for half in range(2):
        drain_rows(first, half)
        drain_rows(second, half)
    with jax.named_scope("settle3a"):
        settle_last(0)
    with jax.named_scope("settle3b"):
        settle_last(1)
    for half in range(2):
        with jax.named_scope("pass3"):
            for s in (0, 2, 1):
                pass_on(third, s, half)
                put_out(s, half, from_x[s], c)
    with jax.named_scope("puts"):
        for _, kind, i in order:
            if kind == "send":
                item_copy(i, False).wait_send()
    for half in range(2):
        with jax.named_scope("gathered3"):
            ag_copy(third, 3, half, x, other, partner).wait_recv()
            put_out(3, half, x, other)
            for s in (0, 2, 1):
                ag_copy(third, 4 + s, half, from_x[s], other, partner).wait_recv()
                put_out(4 + s, half, from_x[s], other)
    with jax.named_scope("drain"):
        for half in range(2):
            drain_sums(half)
            drain_rows(third, half)
        for copy in leaving:
            copy.wait()


def per_device(
    tokens, ffn_gate, ffn_up, ffn_down, query_proj, key_proj, value_proj, outgate_proj, output_proj,
    rank_down, rank_up, decay_bias, head_gain, norm_gain, norm_bias,
):
    operands = (
        tokens, ffn_gate, ffn_up, ffn_down.T, query_proj, key_proj, value_proj, outgate_proj, output_proj.T,
        rank_down.T, rank_up, decay_bias.reshape(1, -1), head_gain.reshape(1, -1), norm_gain, norm_bias,
    )
    items, order = gather_order()
    count = len(items)
    dma = pltpu.SemaphoreType.DMA
    scratch = [pltpu.VMEM(a.shape, a.dtype) for a in operands]
    scratch += [pltpu.VMEM((NZ, NY, SHARD, tiles * LANES), BF16) for pair in WIDTHS for tiles in pair]
    scratch += [
        pltpu.VMEM((ROWS, 1408), F32),
        pltpu.VMEM((ROWS, 768), BF16),
        pltpu.VMEM((ROWS, D), BF16),
        pltpu.VMEM((2, ROWS // 2, D), BF16),
        pltpu.VMEM((ROWS, D), BF16),
        pltpu.VMEM((ROWS, DV), BF16),
        pltpu.VMEM((NZ, 2, NX, OWN, COLS), BF16),
        pltpu.VMEM((NZ, NX, OWN, COLS), BF16),
        pltpu.VMEM((NZ, NX, OWN, COLS), BF16),
        pltpu.VMEM((3, NZ, OWN, COLS), BF16),
        pltpu.VMEM((OWN, D), F32),
        dma((count,)), dma((count,)), dma((15,)),
        dma((2, NZ)), dma((2, NZ)), dma((2, 3, NZ)), dma((2, 3, NZ)), dma((7, 2)), dma((7, 2)), dma((8, 2)),
    ]
    rows = pl.pallas_call(
        functools.partial(layer_kernel, items, order),
        out_shape=jax.ShapeDtypeStruct((ROWS, D), BF16),
        in_specs=[pl.BlockSpec(memory_space=pltpu.HBM)] * 15,
        out_specs=pl.BlockSpec(memory_space=pltpu.HBM),
        scratch_shapes=scratch,
        compiler_params=pltpu.CompilerParams(
            collective_id=0, has_side_effects=True, vmem_limit_bytes=60 * 1024 * 1024),
        name="layer",
    )(*operands)
    return jnp.where(lax.axis_index("tp") >= 0, rows, jnp.zeros_like(rows))


def solution(mesh):
    finer = Mesh(
        mesh.devices.reshape(mesh.shape["rep"], NZ, NY, mesh.shape["tp"]),
        ("rep", "fs_0", "fs_1", "tp"),
    )
    return jax.shard_map(
        per_device,
        mesh=finer,
        in_specs=(
            P(REP_FS, None), P(FS, "tp"), P(FS, "tp"), P("tp", FS), P(FS, "tp"), P(FS, "tp"), P(FS, "tp"),
            P(FS, "tp"), P("tp", FS), P(), P(), P(), P(), P(), P(),
        ),
        out_specs=P(REP_FS, None),
        check_vma=False,
    )
```

```python
import functools
import heapq

import jax
import jax.numpy as jnp
from jax import lax
from jax.experimental import pallas as pl
from jax.experimental.pallas import tpu as pltpu
from jax.sharding import Mesh
from jax.sharding import PartitionSpec as P

DK = 64
DV = 128
FS = ("fs_0", "fs_1")
REP_FS = ("rep", "fs_0", "fs_1")
NZ, NY, NX = 8, 4, 4
ROWS = 256
D = 2048
SHARD = 64
COLS = 256
OWN = 32
LANES = 128

EPSILON = 1e-05
HEAD_FLOOR = 1.0
RESIDUAL_SCALE = 2.0**0.5
GATE_SOFTNESS = 16.0

MESH = pl.DeviceIdType.MESH
F32 = jnp.float32
BF16 = jnp.bfloat16
LINKS = ("z+", "z-", "y+", "y-")
WIDTHS = ((7, 4), (3, 3), (3, 1))
NEAREST = (0, 1, -1, 2, -2, 3, -3, 4)
CHUNK_LATE = (0.0, 3.33, 13.5)
FIRST_Z = (5.8, 6.9, 4.1, 3.2)
THEN_Y = (6.4, 0.0)
FIRST_Y = (8.4, 6.6)
THEN_Z = ((2.7, 6.6, 1.6, -2.6), (3.9, 1.4, 1.8, -1.1), (4.2, 1.6, 5.2, 1.5))
BACKLOG = 2.525
MIDDLES_AT = ((-2.0, 1), (-1.0, 1), (0.0, 1), (1.5, 0))
SETTLE_AT = 4.5
PASS_AT = 11.0


def spot(slot):
    return (slot[0] % NZ, slot[1] % NY)


def gather_items():
    items, groups = [], []

    def add(chunk, part, pair, rise):
        members = []
        for link, slot, half in pair:
            dz, dy = slot
            lands = {"z+": (dz - 1, dy), "z-": (dz + 1, dy), "y+": (dz, dy - 1), "y-": (dz, dy + 1)}[link]
            size = WIDTHS[chunk][part] * (1.0 if half is None else 0.5)
            members.append(len(items))
            items.append((chunk, part, link, slot, half, lands, CHUNK_LATE[chunk] - rise, size, len(groups)))
        groups.append(members)

    def along_z(chunk, part, dy, rise):
        for s in range(4):
            halves = (None, None) if s < 3 else (0, 1)
            add(chunk, part, [("z+", (-s, dy), halves[0]), ("z-", (s, dy), halves[1])], rise[s])

    def along_y(chunk, part, dz, rise):
        add(chunk, part, [("y+", (dz, 0), None), ("y-", (dz, 0), None)], rise[0])
        add(chunk, part, [("y+", (dz, -1), 0), ("y-", (dz, 1), 1)], rise[1])

    for chunk in range(len(WIDTHS)):
        along_z(chunk, 0, 0, FIRST_Z)
        for dz in NEAREST:
            along_y(chunk, 0, dz, THEN_Y)
        along_y(chunk, 1, 0, FIRST_Y)
        for dy in (0, 1, -1, 2):
            along_z(chunk, 1, dy, THEN_Z[abs(dy)])
    return items, groups


def gather_order(tile_us=0.352, fixed=0.05, hop=2.9):
    items, groups = gather_items()
    held = {(c, p, (0, 0)): {0, 1} for c in range(len(WIDTHS)) for p in (0, 1)}
    waiting = list(range(len(items)))
    missing = [len(members) for members in groups]
    ready = {link: [] for link in LINKS}
    free = {link: 0.0 for link in LINKS}
    order, flying = [], []

    def step(now):
        left = []
        for i in waiting:
            chunk, part, link, slot, half = items[i][:5]
            have = held.get((chunk, part, spot(slot)), set())
            if have >= ({0, 1} if half is None else {half}):
                heapq.heappush(ready[link], (items[i][6], i))
            else:
                left.append(i)
        waiting[:] = left
        for link in LINKS:
            while ready[link] and free[link] - now < BACKLOG:
                _, i = heapq.heappop(ready[link])
                free[link] = max(now, free[link]) + items[i][7] * tile_us + fixed
                heapq.heappush(flying, (free[link] + hop, i))
                order.append((now, "send", i))

    step(0.0)
    while flying:
        now, i = heapq.heappop(flying)
        group = items[i][8]
        missing[group] -= 1
        if missing[group]:
            continue
        for k in groups[group]:
            chunk, part, _, _, half, lands = items[k][:6]
            held.setdefault((chunk, part, spot(lands)), set()).update({0, 1} if half is None else {half})
        order.append((now, "land", group))
        step(now)
    return items, groups, order


def dot_nt(a, b):
    return lax.dot_general(a, b, (((1,), (1,)), ((), ())), preferred_element_type=F32)


def dot_nn(a, b, precision=None):
    return lax.dot_general(a, b, (((1,), (0,)), ((), ())), preferred_element_type=F32, precision=precision)


def silu(v):
    return v / (1.0 + jnp.exp(-v))


def boundary(prefix, m):
    if m >= 4:
        parts = prefix.reshape(ROWS // (2 * m), 2 * m, DK)
        edge = jnp.broadcast_to(parts[:, m - 1 : m, :], parts.shape)
        return edge.reshape(ROWS, DK)
    parts = prefix.reshape(ROWS // 8, 8, DK)
    row = lax.broadcasted_iota(jnp.int32, parts.shape, 1)
    edge = jnp.broadcast_to(parts[:, 8 - m - 1 : 8 - m, :], parts.shape)
    for at in range(8 - 4 * m, -1, -2 * m):
        edge = jnp.where(row < at + 2 * m, jnp.broadcast_to(parts[:, at + m - 1 : at + m, :], parts.shape), edge)
    return edge.reshape(ROWS, DK)


def head_out(q, k, v, log_decay):
    row = lax.broadcasted_iota(jnp.int32, (ROWS, ROWS), 0)
    col = lax.broadcasted_iota(jnp.int32, (ROWS, ROWS), 1)
    prefix = dot_nn((col <= row).astype(F32), log_decay, lax.Precision.HIGHEST)
    apart = row ^ col
    scores = jnp.where(row == col, jnp.sum(q * k, axis=1, keepdims=True), 0.0)
    m = ROWS // 2
    while m:
        fade = jnp.exp(-jnp.abs(prefix - boundary(prefix, m)))
        level = dot_nt((q * fade).astype(BF16), (k * fade).astype(BF16))
        scores = jnp.where((row > col) & (apart >= m) & (apart < 2 * m), level, scores)
        m //= 2
    return dot_nn(scores.astype(BF16), v.astype(BF16))


def layer_kernel(items, groups, order, *refs):
    sources = refs[:15]
    out = refs[15]
    staged = refs[16:31]
    (tok, gate, up, down, query, key, value, outgate, output, rank_down, rank_up, bias, head_gain, norm_gain,
     norm_bias) = staged
    (GA, GB, DA, DB, QA, QB, acc, hid, first, second, third, mixed, projected, sendbuf, pairbuf, xsend, xrecv, tot) = refs[31:49]
    (put_sem, get_sem, own_sem, pair_s, pair_r, x_s, x_r, ag_s, ag_r, out_sem) = refs[49:]
    bufs = ((GA, GB), (DA, DB), (QA, QB))
    cuts = [a * LANES for a, _ in WIDTHS]

    rep, zl, y, tp = (lax.axis_index(a) for a in ("rep", "fs_0", "fs_1", "tp"))
    zg = rep * NZ + zl
    x, c = tp // 2, lax.rem(tp, 2)
    other = 1 - c

    def at_z(step):
        g = lax.rem(zg + step + 16, 16)
        return (g // NZ, lax.rem(g, NZ), y, tp)

    def at_y(step):
        return (rep, zl, lax.rem(y + step + NY, NY), tp)

    def at_x(step):
        return (rep, zl, y, lax.rem(x + step + NX, NX) * 2 + c)

    partner = (rep, zl, y, x * 2 + other)
    where = {"z+": at_z(1), "z-": at_z(-1), "y+": at_y(1), "y-": at_y(-1)}
    xs = [at_x(s) for s in (1, 2, 3)]
    from_x = [lax.rem(x - s + NX, NX) for s in (1, 2, 3)]
    z_at = {k: lax.rem(zl + k, NZ) for k in range(NZ)}
    y_at = {k: lax.rem(y + k, NY) for k in range(NY)}

    barrier = pltpu.get_barrier_semaphore()
    friends = list(where.values()) + xs + [partner]
    for friend in friends:
        pl.semaphore_signal(barrier, inc=1, device_id=friend, device_id_type=MESH)
    loads = [pltpu.make_async_copy(a, b, own_sem.at[k]) for k, (a, b) in enumerate(zip(sources, staged))]
    for k in (1, 2, 3, 4, 5, 6, 7, 8, 0, 9, 10, 11, 12, 13, 14):
        loads[k].start()

    mine_at = zl * NY + y

    def pack(pair, cut, at, piece):
        stop = at + piece.shape[1]
        if at < cut:
            pair[0][mine_at, :, at : min(stop, cut)] = piece[:, : min(stop, cut) - at]
        if stop > cut:
            lo = max(at, cut)
            pair[1][mine_at, :, lo - cut : stop - cut] = piece[:, lo - at :]

    def side_by_side(a, b):
        return jnp.concatenate([a.astype(F32), b.astype(F32)], axis=1).astype(BF16)

    with jax.named_scope("pack"):
        for k in range(1, 9):
            loads[k].wait()
        pack(bufs[0], cuts[0], 0, gate[:, 0:640])
        pack(bufs[0], cuts[0], 640, up[:, 0:640])
        pack(bufs[0], cuts[0], 1280, side_by_side(gate[:, 640:704], up[:, 640:704]))
        pack(bufs[1], cuts[1], 0, down[:, 0:640])
        pack(bufs[1], cuts[1], 640, side_by_side(down[:, 640:704], jnp.zeros((SHARD, 64), BF16)))
        pack(bufs[2], cuts[2], 0, side_by_side(query[...], key[...]))
        pack(bufs[2], cuts[2], 128, value[...])
        pack(bufs[2], cuts[2], 256, outgate[...])
        pack(bufs[2], cuts[2], 384, output[...])
    with jax.named_scope("barrier"):
        pl.semaphore_wait(barrier, len(friends))

    def place(chunk, part, slot, half):
        dz, dy = spot(slot)
        at = z_at[dz] * NY + y_at[dy]
        if half is None:
            return bufs[chunk][part].at[at]
        return bufs[chunk][part].at[at, pl.ds(32 * half, 32)]

    def put(i):
        chunk, part, link, slot, half = items[i][:5]
        here = place(chunk, part, slot, half)
        pltpu.make_async_remote_copy(
            src_ref=here, dst_ref=here, send_sem=put_sem.at[2 * chunk + part], recv_sem=get_sem.at[items[i][8]],
            device_id=where[link], device_id_type=MESH).start()

    def bytes_of(chunk, part, slabs, group):
        count = bufs[chunk][part].at[pl.ds(0, slabs)]
        return pltpu.make_async_remote_copy(
            src_ref=count, dst_ref=count, send_sem=put_sem.at[2 * chunk + part], recv_sem=get_sem.at[group],
            device_id=where["z+"], device_id_type=MESH)

    def landed(group):
        chunk, part, _, _, half = items[groups[group][0]][:5]
        bytes_of(chunk, part, 2 if half is None else 1, group).wait_recv()

    def all_put():
        for chunk in range(len(WIDTHS)):
            for part in range(2):
                bytes_of(chunk, part, NZ * NY - 1, 0).wait_send()

    def group_of(buf, zi, count=1):
        return buf[pl.ds(zi * NY, NY * count)].reshape(COLS * count, buf.shape[2])

    def gate_up(zi):
        a = tok[:, pl.ds(pl.multiple_of(zi * COLS, COLS), COLS)]
        acc[:, : cuts[0]] += dot_nn(a, group_of(GA, zi))
        acc[:, cuts[0] :] += dot_nn(a, group_of(GB, zi))

    def clear(rows):
        acc[rows, :] = jnp.zeros((rows.stop - rows.start, 1408), F32)

    def hidden(rows):
        hid[rows, 0:640] = (silu(acc[rows, 0:640]) * acc[rows, 640:1280]).astype(BF16)
        last = acc[rows, 1280:1408]
        lane = lax.broadcasted_iota(jnp.int32, last.shape, 1)
        mixed_last = silu(last) * pltpu.roll(last, 64, 1)
        hid[rows, 640:768] = jnp.where(lane < 64, mixed_last, 0.0).astype(BF16)

    def down_part(rows):
        def part(zi):
            cut = cuts[1]
            return dot_nt(hid[rows, :cut], group_of(DA, zi)) + dot_nt(hid[rows, cut:], group_of(DB, zi))
        return part

    def pair_copy(zi, half):
        if half is None:
            src, dst, sem, out_of = sendbuf.at[zi, other], pairbuf.at[zi], zi, 0
        else:
            rows, both = pl.ds(16 * half, 16), pl.ds(zi, 2)
            src, dst, sem, out_of = sendbuf.at[both, other, :, rows], pairbuf.at[both, :, rows], 4 * half + zi // 2, half
        return pltpu.make_async_remote_copy(
            src_ref=src, dst_ref=dst, send_sem=pair_s.at[out_of], recv_sem=pair_r.at[sem],
            device_id=partner, device_id_type=MESH)

    def x_copy(zi, s, half):
        to = lax.rem(x + s + 1, NX)
        if half is None:
            src, dst, sem = xsend.at[zi, to], xrecv.at[s, zi], 0
        else:
            rows, both = pl.ds(16 * half, 16), pl.ds(zi, 2)
            src, dst, sem = xsend.at[both, to, rows], xrecv.at[s, both, rows], half
        return pltpu.make_async_remote_copy(
            src_ref=src, dst_ref=dst, send_sem=x_s.at[sem, s], recv_sem=x_r.at[sem, s],
            device_id=xs[s], device_id_type=MESH)

    def sums_of(half, s):
        rows = pl.ds(0, OWN) if half is None else pl.ds(16 * half, 16)
        sem = 0 if half is None else half
        ref = xrecv.at[s, :, rows]
        return pltpu.make_async_remote_copy(
            src_ref=ref, dst_ref=ref, send_sem=x_s.at[sem, s], recv_sem=x_r.at[sem, s],
            device_id=xs[s], device_id_type=MESH)

    def middle(zi, half):
        pair_copy(zi, half).wait_recv()
        if half is None:
            xsend[zi] = (sendbuf[zi, c].astype(F32) + pairbuf[zi].astype(F32)).astype(BF16)
        else:
            rows = slice(16 * half, 16 * half + 16)
            for k in range(2):
                xsend[zi + k, :, rows] = (
                    sendbuf[zi + k, c, :, rows].astype(F32) + pairbuf[zi + k, :, rows].astype(F32)
                ).astype(BF16)
        for s in (1, 0, 2):
            x_copy(zi, s, half).start()

    def settle(residual, store, factor, which, half):
        rows = slice(0, OWN) if half is None else slice(16 * half, 16 * half + 16)
        for s in range(3):
            sums_of(half, s).wait_recv()
        own = residual.astype(F32)
        total = 0.0
        for zi in range(NZ):
            part = sendbuf[zi, c, x, rows].astype(F32) + pairbuf[zi, x, rows].astype(F32)
            for s in range(3):
                part = part + xrecv[s, zi, rows].astype(F32)
            part = RESIDUAL_SCALE * own[:, zi * COLS : (zi + 1) * COLS] + factor * part
            tot[rows, zi * COLS : (zi + 1) * COLS] = part
            total = total + jnp.sum(part, axis=1, keepdims=True)
        centred = tot[rows, :] - total * (1.0 / D)
        spread = jnp.mean(centred * centred, axis=1, keepdims=True)
        normed = centred * lax.rsqrt(spread + EPSILON) * norm_gain[which : which + 1, :] + norm_bias[which : which + 1, :]
        store(normed.astype(BF16))

    def block(target, xx, cc, half):
        t = xx * 2 + cc
        if target is not third and target is not out:
            return target.at[half, pl.ds(pl.multiple_of(t * 16, 16), 16)]
        return target.at[pl.ds(pl.multiple_of(t * OWN + 16 * half, 16), 16)]

    def ag_copy(target, k, half, xx, cc, to):
        ref = block(target, xx, cc, half)
        return pltpu.make_async_remote_copy(
            src_ref=ref, dst_ref=ref, send_sem=ag_s.at[half], recv_sem=ag_r.at[k, half],
            device_id=to, device_id_type=MESH)

    def spread_out(target, half):
        for s in (1, 0, 2):
            ag_copy(target, s, half, x, c, xs[s]).start()
        ag_copy(target, 3, half, x, c, partner).start()

    def pass_on(target, s, half):
        ag_copy(target, s, half, from_x[s], c, xs[s]).wait_recv()
        ag_copy(target, 4 + s, half, from_x[s], c, partner).start()

    def pass_all(target, half):
        for s in (0, 2, 1):
            pass_on(target, s, half)

    def gathered(target, half):
        ag_copy(target, 3, half, x, other, partner).wait_recv()
        for s in range(3):
            ag_copy(target, 4 + s, half, from_x[s], other, partner).wait_recv()

    def drain_rows(half):
        ref = second.at[0, pl.ds(0, 112)]
        pltpu.make_async_remote_copy(
            src_ref=ref, dst_ref=ref, send_sem=ag_s.at[half], recv_sem=ag_r.at[0, half],
            device_id=partner, device_id_type=MESH).wait_send()

    def drain_sums(half):
        rows = pl.ds(0, OWN) if half is None else pl.ds(16 * half, 16)
        ref = pairbuf.at[:, :, rows]
        pltpu.make_async_remote_copy(
            src_ref=ref, dst_ref=ref, send_sem=pair_s.at[0 if half is None else half], recv_sem=pair_r.at[0],
            device_id=partner, device_id_type=MESH).wait_send()
        for s in range(3):
            sums_of(half, s).wait_send()

    every = slice(0, ROWS)
    row0 = pl.multiple_of(tp * OWN, OWN)
    held = {}
    done_groups = [[], [], []]
    state = {"gate": 0, "fronts": [], "middles": []}
    end_of = [max(t for t, kind, g in order if kind == "land" and items[groups[g][0]][0] == k) for k in range(3)]
    steps = [(t, 0, kind, i) for t, kind, i in order]
    steps += [(end_of[1] + at, 1, "middles", keep) for at, keep in MIDDLES_AT]
    steps += [(end_of[1] + SETTLE_AT, 2, "settle", 0)]
    steps += [(end_of[1] + PASS_AT + 2.5 * half, 3, "pass", half) for half in range(2)]
    steps.sort(key=lambda e: e[:2])
    clear(every)
    loads[0].wait()
    for k in range(9, 15):
        loads[k].wait()

    def first_front(zi):
        value = down_part(every)(zi)
        for t in range(8):
            sendbuf[zi, t % 2, t // 2] = value[t * OWN : (t + 1) * OWN].astype(BF16)
        pair_copy(zi, None).start()

    def flush_middles(keep):
        while len(state["middles"]) > keep:
            with jax.named_scope("mid1"):
                middle(state["middles"].pop(0), None)

    for now, _, kind, what in steps:
        if kind == "send":
            put(what)
        elif kind == "land":
            chunk = items[groups[what][0]][0]
            with jax.named_scope("land%d" % chunk):
                landed(what)
            for i in groups[what]:
                half, lands = items[i][4:6]
                key_ = (chunk, spot(lands)[0])
                held[key_] = held.get(key_, 0.0) + (1.0 if half is None else 0.5)
                if held[key_] == (6.0 if spot(lands)[0] == 0 else 8.0):
                    done_groups[chunk].append(spot(lands)[0])
            for k in done_groups[0][state["gate"] :]:
                with jax.named_scope("gu_a"):
                    gate_up(z_at[k])
                state["gate"] += 1
                if state["gate"] == NZ:
                    with jax.named_scope("gu_b"):
                        hidden(every)
            if state["gate"] == NZ:
                for k in done_groups[1]:
                    if k not in state["fronts"]:
                        state["fronts"].append(k)
                        with jax.named_scope("front1"):
                            first_front(z_at[k])
                        state["middles"].append(z_at[k])
        elif kind == "middles":
            flush_middles(what)
        elif kind == "settle":
            def store_first(normed):
                for half in range(2):
                    first[half, pl.ds(pl.multiple_of(tp * 16, 16), 16), :] = normed[16 * half : 16 * half + 16]
            with jax.named_scope("settle1"):
                settle(tok[pl.ds(row0, OWN), :], store_first, 0.5, 0, None)
            spread_out(first, 0)
            spread_out(first, 1)
        else:
            with jax.named_scope("pass1"):
                pass_all(first, what)

    for half in range(2):
        with jax.named_scope("gathered1"):
            gathered(first, half)
        with jax.named_scope("proj"):
            rows = first[half]
            pieces = [dot_nn(rows, QA[...].reshape(D, cuts[2]))]
            if cuts[2] < 384:
                pieces.append(dot_nn(rows, QB[:, :, : 384 - cuts[2]].reshape(D, 384 - cuts[2])))
            pieces.append(dot_nt(rows, rank_down[...]))
            at = 0
            for piece in pieces:
                wide = piece.shape[1]
                for t in range(8):
                    projected[t * OWN + 16 * half : t * OWN + 16 * half + 16, at : at + wide] = piece[t * 16 : t * 16 + 16]
                at += wide
    with jax.named_scope("decay"):
        ranks = projected[:, 384:400]
        pair_at = pl.multiple_of(x * 128, 128)

        def mine(ref):
            both = ref[:, pl.ds(pair_at, 128)].astype(F32)
            return jnp.where(c == 0, both[:, :64], both[:, 64:])
        source = dot_nn(ranks, mine(rank_up), lax.Precision.HIGHEST) + mine(bias)
        log_decay = (jnp.minimum(source, 0.0) - jnp.log1p(jnp.exp(-jnp.abs(source)))) * (1.0 / GATE_SOFTNESS)
    with jax.named_scope("gla"):
        heads = head_out(projected[:, :DK] * DK**-0.5, projected[:, DK : 2 * DK], projected[:, 128:256], log_decay)
        scale = lax.rsqrt(jnp.mean(heads * heads, axis=1, keepdims=True) + HEAD_FLOOR)
        gain = head_gain[:, pl.ds(pl.multiple_of(tp * DV, DV), DV)]
        mixed[...] = (heads * scale * gain * silu(projected[:, 256:384])).astype(BF16)
    drain_sums(None)
    for half in range(2):
        drain_rows(half)

    def output_fronts(k):
        part = dot_nt(mixed[...], group_of(QB, 4 * k, 4)[:, -128:])
        for g in range(4):
            for t in range(8):
                sendbuf[4 * k + g, t % 2, t // 2] = part[
                    t * OWN : (t + 1) * OWN, g * COLS : (g + 1) * COLS].astype(BF16)
        for half in range(2):
            for g in range(0, 4, 2):
                pair_copy(4 * k + g, half).start()

    def middles(half, lo, hi):
        def step(k, carry):
            middle(2 * k, half)
            return carry
        lax.fori_loop(lo, hi, step, 0)

    with jax.named_scope("rs2"):
        output_fronts(0)
        output_fronts(1)
        middles(0, 0, 4)
        middles(1, 0, 4)

    def put_out(half, xx, cc):
        pltpu.make_async_copy(block(third, xx, cc, half), block(out, xx, cc, half), out_sem.at[0]).start()

    def settle_second(half):
        def store(normed):
            second[half, pl.ds(pl.multiple_of(tp * 16, 16), 16), :] = normed
        settle(first[half, pl.ds(pl.multiple_of(tp * 16, 16), 16), :], store, 1.0, 1, half)
        spread_out(second, half)

    def settle_last(half):
        def store(normed):
            third[pl.ds(pl.multiple_of(row0 + 16 * half, 16), 16), :] = normed
        settle(second[half, pl.ds(pl.multiple_of(tp * 16, 16), 16), :], store, 0.5, 2, half)
        spread_out(third, half)
        put_out(half, x, c)

    def rows_of(half):
        return slice(128 * half, 128 * half + 128)

    def mixer_front(half):
        rows = rows_of(half)
        acc[rows, : cuts[0]] = dot_nn(second[half], GA[...].reshape(D, cuts[0]))
        acc[rows, cuts[0] :] = dot_nn(second[half], GB[...].reshape(D, 1408 - cuts[0]))
        hidden(rows)

    def down_sums(half):
        rows, cut = rows_of(half), cuts[1]
        for k in range(2):
            part = dot_nt(hid[rows, :cut], group_of(DA, 4 * k, 4)) + dot_nt(hid[rows, cut:], group_of(DB, 4 * k, 4))
            for g in range(4):
                for t in range(8):
                    sendbuf[4 * k + g, t % 2, t // 2, 16 * half : 16 * half + 16] = part[
                        t * 16 : (t + 1) * 16, g * COLS : (g + 1) * COLS].astype(BF16)
            for g in range(0, 4, 2):
                pair_copy(4 * k + g, half).start()
        middles(half, 0, 4)

    with jax.named_scope("settle2a"):
        settle_second(0)
    with jax.named_scope("settle2b"):
        settle_second(1)
    with jax.named_scope("pass2a"):
        pass_all(second, 0)
        gathered(second, 0)
    with jax.named_scope("gu2a"):
        mixer_front(0)
    with jax.named_scope("pass2b"):
        pass_all(second, 1)
    with jax.named_scope("rs3a"):
        drain_sums(0)
        down_sums(0)
    with jax.named_scope("gathered2b"):
        gathered(second, 1)
    with jax.named_scope("gu2b"):
        mixer_front(1)
    with jax.named_scope("rs3b"):
        drain_sums(1)
        down_sums(1)
    for half in range(2):
        drain_rows(half)
    with jax.named_scope("settle3a"):
        settle_last(0)
    with jax.named_scope("settle3b"):
        settle_last(1)
    for half in range(2):
        with jax.named_scope("pass3"):
            for s in (0, 2, 1):
                pass_on(third, s, half)
                put_out(half, from_x[s], c)
    with jax.named_scope("puts"):
        all_put()
    for half in range(2):
        with jax.named_scope("gathered3"):
            ag_copy(third, 3, half, x, other, partner).wait_recv()
            put_out(half, x, other)
            for s in (0, 2, 1):
                ag_copy(third, 4 + s, half, from_x[s], other, partner).wait_recv()
                put_out(half, from_x[s], other)
    with jax.named_scope("drain"):
        for half in range(2):
            drain_sums(half)
            drain_rows(half)
        pltpu.make_async_copy(third, out, out_sem.at[0]).wait()


def per_device(
    tokens, ffn_gate, ffn_up, ffn_down, query_proj, key_proj, value_proj, outgate_proj, output_proj,
    rank_down, rank_up, decay_bias, head_gain, norm_gain, norm_bias,
):
    operands = (
        tokens, ffn_gate, ffn_up, ffn_down.T, query_proj, key_proj, value_proj, outgate_proj, output_proj.T,
        rank_down.T, rank_up, decay_bias.reshape(1, -1), head_gain.reshape(1, -1), norm_gain, norm_bias,
    )
    items, groups, order = gather_order()
    dma = pltpu.SemaphoreType.DMA
    scratch = [pltpu.VMEM(a.shape, a.dtype) for a in operands]
    scratch += [pltpu.VMEM((NZ * NY, SHARD, tiles * LANES), BF16) for pair in WIDTHS for tiles in pair]
    scratch += [
        pltpu.VMEM((ROWS, 1408), F32),
        pltpu.VMEM((ROWS, 768), BF16),
        pltpu.VMEM((2, ROWS // 2, D), BF16),
        pltpu.VMEM((2, ROWS // 2, D), BF16),
        pltpu.VMEM((ROWS, D), BF16),
        pltpu.VMEM((ROWS, DV), BF16),
        pltpu.VMEM((ROWS, 512), F32),
        pltpu.VMEM((NZ, 2, NX, OWN, COLS), BF16),
        pltpu.VMEM((NZ, NX, OWN, COLS), BF16),
        pltpu.VMEM((NZ, NX, OWN, COLS), BF16),
        pltpu.VMEM((3, NZ, OWN, COLS), BF16),
        pltpu.VMEM((OWN, D), F32),
        dma((2 * len(WIDTHS),)), dma((len(groups),)), dma((15,)),
        dma((2,)), dma((NZ,)), dma((2, 3)), dma((2, 3)), dma((2,)), dma((7, 2)), dma((1,)),
    ]
    rows = pl.pallas_call(
        functools.partial(layer_kernel, items, groups, order),
        out_shape=jax.ShapeDtypeStruct((ROWS, D), BF16),
        in_specs=[pl.BlockSpec(memory_space=pltpu.HBM)] * 15,
        out_specs=pl.BlockSpec(memory_space=pltpu.HBM),
        scratch_shapes=scratch,
        compiler_params=pltpu.CompilerParams(
            collective_id=0, has_side_effects=True, vmem_limit_bytes=60 * 1024 * 1024),
        name="layer",
    )(*operands)
    return jnp.where(lax.axis_index("tp") >= 0, rows, jnp.zeros_like(rows))


def solution(mesh):
    finer = Mesh(
        mesh.devices.reshape(mesh.shape["rep"], NZ, NY, mesh.shape["tp"]),
        ("rep", "fs_0", "fs_1", "tp"),
    )
    return jax.shard_map(
        per_device,
        mesh=finer,
        in_specs=(
            P(REP_FS, None), P(FS, "tp"), P(FS, "tp"), P("tp", FS), P(FS, "tp"), P(FS, "tp"), P(FS, "tp"),
            P(FS, "tp"), P("tp", FS), P(), P(), P(), P(), P(), P(),
        ),
        out_specs=P(REP_FS, None),
        check_vma=False,
    )
```

```python
import functools
import heapq

import jax
import jax.numpy as jnp
from jax import lax
from jax.experimental import pallas as pl
from jax.experimental.pallas import tpu as pltpu
from jax.sharding import Mesh
from jax.sharding import PartitionSpec as P

DK = 64
DV = 128
FS = ("fs_0", "fs_1")
REP_FS = ("rep", "fs_0", "fs_1")
NZ, NY, NX = 8, 4, 4
ROWS = 256
D = 2048
SHARD = 64
COLS = 256
OWN = 32
HALF = 128
LANES = 128

EPSILON = 1e-05
HEAD_FLOOR = 1.0
RESIDUAL_SCALE = 2.0**0.5
GATE_SOFTNESS = 16.0

MESH = pl.DeviceIdType.MESH
F32 = jnp.float32
BF16 = jnp.bfloat16
LINKS = ("z+", "z-", "y+", "y-")
WIDTHS = ((7, 4), (3, 3), (3, 1))
NEAREST = (0, 1, -1, 2, -2, 3, -3, 4)
CHUNK_LATE = (0.0, 3.33, 13.5)
FIRST_Z = (5.8, 6.9, 4.1, 3.2)
THEN_Y = (6.4, 0.0)
FIRST_Y = (8.4, 6.6)
THEN_Z = ((2.7, 6.6, 1.6, -2.6), (3.9, 1.4, 1.8, -1.1), (4.2, 1.6, 5.2, 1.5))
BACKLOG = 2.525
MIDDLES_AT = ((-2.0, 1), (-1.0, 1), (0.0, 1), (1.5, 0))
SETTLE_AT = 4.5
PASS_AT = 10.5


def spot(slot):
    return (slot[0] % NZ, slot[1] % NY)


def gather_items():
    items, groups = [], []

    shared = {}

    def add(chunk, part, pair, rise, share=None):
        if share is None or (chunk, part, share) not in shared:
            shared[chunk, part, share] = len(groups)
            groups.append([])
        group = shared[chunk, part, share]
        for link, slot, half in pair:
            dz, dy = slot
            lands = {"z+": (dz - 1, dy), "z-": (dz + 1, dy), "y+": (dz, dy - 1), "y-": (dz, dy + 1)}[link]
            size = WIDTHS[chunk][part] * (1.0 if half is None else 0.5)
            groups[group].append(len(items))
            items.append((chunk, part, link, slot, half, lands, CHUNK_LATE[chunk] - rise, size, group))

    def along_z(chunk, part, dy, rise):
        for s in range(4):
            halves = (None, None) if s < 3 else (0, 1)
            share = "ends" if part == 1 and s == 3 else None
            add(chunk, part, [("z+", (-s, dy), halves[0]), ("z-", (s, dy), halves[1])], rise[s], share)

    def along_y(chunk, part, dz, rise):
        add(chunk, part, [("y+", (dz, 0), None), ("y-", (dz, 0), None)], rise[0])
        share = None if part == 1 else abs(dz) if chunk < 2 else 0
        add(chunk, part, [("y+", (dz, -1), 0), ("y-", (dz, 1), 1)], rise[1], share)

    for chunk in range(len(WIDTHS)):
        along_z(chunk, 0, 0, FIRST_Z)
        for dz in NEAREST:
            along_y(chunk, 0, dz, THEN_Y)
        along_y(chunk, 1, 0, FIRST_Y)
        for dy in (0, 1, -1, 2):
            along_z(chunk, 1, dy, THEN_Z[abs(dy)])
    return items, groups


def gather_order(tile_us=0.352, fixed=0.05, hop=2.9):
    items, groups = gather_items()
    held = {(c, p, (0, 0)): {0, 1} for c in range(len(WIDTHS)) for p in (0, 1)}
    waiting = list(range(len(items)))
    missing = [len(members) for members in groups]
    ready = {link: [] for link in LINKS}
    free = {link: 0.0 for link in LINKS}
    order, flying = [], []

    def step(now):
        left = []
        for i in waiting:
            chunk, part, link, slot, half = items[i][:5]
            have = held.get((chunk, part, spot(slot)), set())
            if have >= ({0, 1} if half is None else {half}):
                heapq.heappush(ready[link], (items[i][6], i))
            else:
                left.append(i)
        waiting[:] = left
        for link in LINKS:
            while ready[link] and free[link] - now < BACKLOG:
                _, i = heapq.heappop(ready[link])
                free[link] = max(now, free[link]) + items[i][7] * tile_us + fixed
                heapq.heappush(flying, (free[link] + hop, i))
                order.append((now, "send", i))

    step(0.0)
    while flying:
        now, i = heapq.heappop(flying)
        group = items[i][8]
        missing[group] -= 1
        if missing[group]:
            continue
        for k in groups[group]:
            chunk, part, _, _, half, lands = items[k][:6]
            held.setdefault((chunk, part, spot(lands)), set()).update({0, 1} if half is None else {half})
        order.append((now, "land", group))
        step(now)
    return items, groups, order


def dot_nt(a, b):
    return lax.dot_general(a, b, (((1,), (1,)), ((), ())), preferred_element_type=F32)


def dot_nn(a, b, precision=None):
    return lax.dot_general(a, b, (((1,), (0,)), ((), ())), preferred_element_type=F32, precision=precision)


def silu(v):
    return v / (1.0 + jnp.exp(-v))


def boundary(prefix, m):
    if m >= 4:
        parts = prefix.reshape(HALF // (2 * m), 2 * m, DK)
        edge = jnp.broadcast_to(parts[:, m - 1 : m, :], parts.shape)
        return edge.reshape(HALF, DK)
    parts = prefix.reshape(HALF // 8, 8, DK)
    row = lax.broadcasted_iota(jnp.int32, parts.shape, 1)
    edge = jnp.broadcast_to(parts[:, 8 - m - 1 : 8 - m, :], parts.shape)
    for at in range(8 - 4 * m, -1, -2 * m):
        edge = jnp.where(row < at + 2 * m, jnp.broadcast_to(parts[:, at + m - 1 : at + m, :], parts.shape), edge)
    return edge.reshape(HALF, DK)


def head_out(q, k, v, log_decay):
    row = lax.broadcasted_iota(jnp.int32, (HALF, HALF), 0)
    col = lax.broadcasted_iota(jnp.int32, (HALF, HALF), 1)
    prefix = dot_nn((col <= row).astype(F32), log_decay, lax.Precision.HIGHEST)
    apart = row ^ col
    scores = jnp.broadcast_to(jnp.sum(q * k, axis=1, keepdims=True), apart.shape)
    m = 1
    while m < HALF:
        fade = jnp.exp(-jnp.abs(prefix - boundary(prefix, m)))
        level = dot_nt((q * fade).astype(BF16), (k * fade).astype(BF16))
        scores = jnp.where(apart >= m, level, scores)
        m *= 2
    scores = jnp.where(row >= col, scores, 0.0)
    return dot_nn(scores.astype(BF16), v.astype(BF16)), prefix


def layer_kernel(items, groups, order, *refs):
    sources = refs[:15]
    out = refs[15]
    staged = refs[16:31]
    (tok, gate, up, down, query, key, value, outgate, output, rank_down, rank_up, bias, head_gain, norm_gain,
     norm_bias) = staged
    (GA, GB, DA, DB, QA, QB, acc, hid, first, second, third, mixed, projected, sendbuf, pairbuf, xsend, xrecv, tot) = refs[31:49]
    (put_sem, get_sem, own_sem, pair_s, pair_r, x_s, x_r, ag_s, ag_r, out_sem) = refs[49:]
    bufs = ((GA, GB), (DA, DB), (QA, QB))
    cuts = [a * LANES for a, _ in WIDTHS]

    rep, zl, y, tp = (lax.axis_index(a) for a in ("rep", "fs_0", "fs_1", "tp"))
    zg = rep * NZ + zl
    x, c = tp // 2, lax.rem(tp, 2)
    other = 1 - c

    def at_z(step):
        g = lax.rem(zg + step + 16, 16)
        return (g // NZ, lax.rem(g, NZ), y, tp)

    def at_y(step):
        return (rep, zl, lax.rem(y + step + NY, NY), tp)

    def at_x(step):
        return (rep, zl, y, lax.rem(x + step + NX, NX) * 2 + c)

    partner = (rep, zl, y, x * 2 + other)
    where = {"z+": at_z(1), "z-": at_z(-1), "y+": at_y(1), "y-": at_y(-1)}
    xs = [at_x(s) for s in (1, 2, 3)]
    from_x = [lax.rem(x - s + NX, NX) for s in (1, 2, 3)]
    z_at = {k: lax.rem(zl + k, NZ) for k in range(NZ)}
    y_at = {k: lax.rem(y + k, NY) for k in range(NY)}

    barrier = pltpu.get_barrier_semaphore()
    friends = list(where.values()) + xs + [partner]
    for friend in friends:
        pl.semaphore_signal(barrier, inc=1, device_id=friend, device_id_type=MESH)
    loads = [pltpu.make_async_copy(a, b, own_sem.at[k]) for k, (a, b) in enumerate(zip(sources, staged))]
    for k in (1, 2, 3, 4, 5, 6, 7, 8, 0, 9, 10, 11, 12, 13, 14):
        loads[k].start()

    mine_at = zl * NY + y

    def pack(pair, cut, at, piece):
        stop = at + piece.shape[1]
        if at < cut:
            pair[0][mine_at, :, at : min(stop, cut)] = piece[:, : min(stop, cut) - at]
        if stop > cut:
            lo = max(at, cut)
            pair[1][mine_at, :, lo - cut : stop - cut] = piece[:, lo - at :]

    def side_by_side(a, b):
        return jnp.concatenate([a.astype(F32), b.astype(F32)], axis=1).astype(BF16)

    with jax.named_scope("pack"):
        for k in range(1, 9):
            loads[k].wait()
        pack(bufs[0], cuts[0], 0, gate[:, 0:640])
        pack(bufs[0], cuts[0], 640, up[:, 0:640])
        pack(bufs[0], cuts[0], 1280, side_by_side(gate[:, 640:704], up[:, 640:704]))
        pack(bufs[1], cuts[1], 0, down[:, 0:640])
        pack(bufs[1], cuts[1], 640, side_by_side(down[:, 640:704], jnp.zeros((SHARD, 64), BF16)))
        pack(bufs[2], cuts[2], 0, side_by_side(query[...], key[...]))
        pack(bufs[2], cuts[2], 128, value[...])
        pack(bufs[2], cuts[2], 256, outgate[...])
        pack(bufs[2], cuts[2], 384, output[...])
    with jax.named_scope("barrier"):
        pl.semaphore_wait(barrier, len(friends))

    def place(chunk, part, slot, half):
        dz, dy = spot(slot)
        at = z_at[dz] * NY + y_at[dy]
        if half is None:
            return bufs[chunk][part].at[at]
        return bufs[chunk][part].at[at, pl.ds(32 * half, 32)]

    def put(i):
        chunk, part, link, slot, half = items[i][:5]
        here = place(chunk, part, slot, half)
        pltpu.make_async_remote_copy(
            src_ref=here, dst_ref=here, send_sem=put_sem.at[2 * chunk + part], recv_sem=get_sem.at[items[i][8]],
            device_id=where[link], device_id_type=MESH).start()

    def bytes_of(chunk, part, slabs, group):
        count = bufs[chunk][part].at[pl.ds(0, slabs)]
        return pltpu.make_async_remote_copy(
            src_ref=count, dst_ref=count, send_sem=put_sem.at[2 * chunk + part], recv_sem=get_sem.at[group],
            device_id=where["z+"], device_id_type=MESH)

    def landed(group):
        chunk, part = items[groups[group][0]][:2]
        slabs = sum(2 if items[i][4] is None else 1 for i in groups[group]) // 2
        bytes_of(chunk, part, slabs, group).wait_recv()

    def all_put():
        for chunk in range(len(WIDTHS)):
            for part in range(2):
                bytes_of(chunk, part, NZ * NY - 1, 0).wait_send()

    def group_of(buf, zi, count=1):
        return buf[pl.ds(zi * NY, NY * count)].reshape(COLS * count, buf.shape[2])

    def gate_up(zi):
        a = tok[:, pl.ds(pl.multiple_of(zi * COLS, COLS), COLS)]
        acc[:, : cuts[0]] += dot_nn(a, group_of(GA, zi))
        acc[:, cuts[0] :] += dot_nn(a, group_of(GB, zi))

    def clear(rows):
        acc[rows, :] = jnp.zeros((rows.stop - rows.start, 1408), F32)

    def hidden(rows):
        hid[rows, 0:640] = (silu(acc[rows, 0:640]) * acc[rows, 640:1280]).astype(BF16)
        last = acc[rows, 1280:1408]
        lane = lax.broadcasted_iota(jnp.int32, last.shape, 1)
        mixed_last = silu(last) * pltpu.roll(last, 64, 1)
        hid[rows, 640:768] = jnp.where(lane < 64, mixed_last, 0.0).astype(BF16)

    def down_part(rows):
        def part(zi):
            cut = cuts[1]
            return dot_nt(hid[rows, :cut], group_of(DA, zi)) + dot_nt(hid[rows, cut:], group_of(DB, zi))
        return part

    def pair_copy(zi, half):
        if half is None:
            src, dst, sem, out_of = sendbuf.at[zi, other], pairbuf.at[zi], zi, 0
        else:
            rows, both = pl.ds(16 * half, 16), pl.ds(zi, 2)
            src, dst, sem, out_of = sendbuf.at[both, other, :, rows], pairbuf.at[both, :, rows], 4 * half + zi // 2, half
        return pltpu.make_async_remote_copy(
            src_ref=src, dst_ref=dst, send_sem=pair_s.at[out_of], recv_sem=pair_r.at[sem],
            device_id=partner, device_id_type=MESH)

    def x_copy(zi, s, half):
        to = lax.rem(x + s + 1, NX)
        if half is None:
            src, dst, sem = xsend.at[zi, to], xrecv.at[s, zi], 0
        else:
            rows, both = pl.ds(16 * half, 16), pl.ds(zi, 2)
            src, dst, sem = xsend.at[both, to, rows], xrecv.at[s, both, rows], half
        return pltpu.make_async_remote_copy(
            src_ref=src, dst_ref=dst, send_sem=x_s.at[sem, s], recv_sem=x_r.at[sem, s],
            device_id=xs[s], device_id_type=MESH)

    def sums_of(half, s):
        rows = pl.ds(0, OWN) if half is None else pl.ds(16 * half, 16)
        sem = 0 if half is None else half
        ref = xrecv.at[s, :, rows]
        return pltpu.make_async_remote_copy(
            src_ref=ref, dst_ref=ref, send_sem=x_s.at[sem, s], recv_sem=x_r.at[sem, s],
            device_id=xs[s], device_id_type=MESH)

    def middle(zi, half):
        pair_copy(zi, half).wait_recv()
        if half is None:
            xsend[zi] = (sendbuf[zi, c].astype(F32) + pairbuf[zi].astype(F32)).astype(BF16)
        else:
            rows = slice(16 * half, 16 * half + 16)
            for k in range(2):
                xsend[zi + k, :, rows] = (
                    sendbuf[zi + k, c, :, rows].astype(F32) + pairbuf[zi + k, :, rows].astype(F32)
                ).astype(BF16)
        for s in (1, 0, 2):
            x_copy(zi, s, half).start()

    def settle(residual, store, factor, which, half):
        rows = slice(0, OWN) if half is None else slice(16 * half, 16 * half + 16)
        for s in range(3):
            sums_of(half, s).wait_recv()
        own = residual.astype(F32)
        total = 0.0
        for zi in range(NZ):
            part = sendbuf[zi, c, x, rows].astype(F32) + pairbuf[zi, x, rows].astype(F32)
            for s in range(3):
                part = part + xrecv[s, zi, rows].astype(F32)
            part = RESIDUAL_SCALE * own[:, zi * COLS : (zi + 1) * COLS] + factor * part
            tot[rows, zi * COLS : (zi + 1) * COLS] = part
            total = total + jnp.sum(part, axis=1, keepdims=True)
        centred = tot[rows, :] - total * (1.0 / D)
        spread = jnp.mean(centred * centred, axis=1, keepdims=True)
        normed = centred * lax.rsqrt(spread + EPSILON) * norm_gain[which : which + 1, :] + norm_bias[which : which + 1, :]
        store(normed.astype(BF16))

    def block(target, xx, cc, half):
        t = xx * 2 + cc
        if target is not third and target is not out:
            return target.at[half, pl.ds(pl.multiple_of(t * 16, 16), 16)]
        return target.at[pl.ds(pl.multiple_of(t * 16 + HALF * half, 16), 16)]

    def ag_copy(target, k, half, xx, cc, to):
        ref = block(target, xx, cc, half)
        return pltpu.make_async_remote_copy(
            src_ref=ref, dst_ref=ref, send_sem=ag_s.at[half], recv_sem=ag_r.at[k, half],
            device_id=to, device_id_type=MESH)

    def spread_out(target, half):
        for s in (1, 0, 2):
            ag_copy(target, s, half, x, c, xs[s]).start()
        ag_copy(target, 3, half, x, c, partner).start()

    def pass_on(target, s, half):
        ag_copy(target, s, half, from_x[s], c, xs[s]).wait_recv()
        ag_copy(target, 4 + s, half, from_x[s], c, partner).start()

    def pass_all(target, half):
        for s in (0, 2, 1):
            pass_on(target, s, half)

    def gathered(target, half):
        ag_copy(target, 3, half, x, other, partner).wait_recv()
        for s in range(3):
            ag_copy(target, 4 + s, half, from_x[s], other, partner).wait_recv()

    def drain_rows(half):
        ref = second.at[0, pl.ds(0, 112)]
        pltpu.make_async_remote_copy(
            src_ref=ref, dst_ref=ref, send_sem=ag_s.at[half], recv_sem=ag_r.at[0, half],
            device_id=partner, device_id_type=MESH).wait_send()

    def drain_sums(half):
        rows = pl.ds(0, OWN) if half is None else pl.ds(16 * half, 16)
        ref = pairbuf.at[:, :, rows]
        pltpu.make_async_remote_copy(
            src_ref=ref, dst_ref=ref, send_sem=pair_s.at[0 if half is None else half], recv_sem=pair_r.at[0],
            device_id=partner, device_id_type=MESH).wait_send()
        for s in range(3):
            sums_of(half, s).wait_send()

    every = slice(0, ROWS)
    held = {}
    done_groups = [[], [], []]
    state = {"gate": 0, "fronts": [], "middles": []}
    end_of = [max(t for t, kind, g in order if kind == "land" and items[groups[g][0]][0] == k) for k in range(3)]
    steps = [(t, 0, kind, i) for t, kind, i in order]
    steps += [(end_of[1] + at, 1, "middles", keep) for at, keep in MIDDLES_AT]
    steps += [(end_of[1] + SETTLE_AT, 2, "settle", 0)]
    steps += [(end_of[1] + PASS_AT, 3, "pass", 0)]
    steps.sort(key=lambda e: e[:2])
    clear(every)
    loads[0].wait()
    for k in range(9, 15):
        loads[k].wait()

    def first_front(zi):
        value = down_part(every)(zi)
        for t in range(8):
            for half in range(2):
                at = HALF * half + 16 * t
                sendbuf[zi, t % 2, t // 2, 16 * half : 16 * half + 16] = value[at : at + 16].astype(BF16)
        pair_copy(zi, None).start()

    def flush_middles(keep):
        while len(state["middles"]) > keep:
            with jax.named_scope("mid1"):
                middle(state["middles"].pop(0), None)

    for now, _, kind, what in steps:
        if kind == "send":
            put(what)
        elif kind == "land":
            chunk = items[groups[what][0]][0]
            with jax.named_scope("land%d" % chunk):
                landed(what)
            for i in groups[what]:
                half, lands = items[i][4:6]
                key_ = (chunk, spot(lands)[0])
                held[key_] = held.get(key_, 0.0) + (1.0 if half is None else 0.5)
                if held[key_] == (6.0 if spot(lands)[0] == 0 else 8.0):
                    done_groups[chunk].append(spot(lands)[0])
            for k in done_groups[0][state["gate"] :]:
                with jax.named_scope("gu_a"):
                    gate_up(z_at[k])
                state["gate"] += 1
                if state["gate"] == NZ:
                    with jax.named_scope("gu_b"):
                        hidden(every)
            if state["gate"] == NZ:
                for k in done_groups[1]:
                    if k not in state["fronts"]:
                        state["fronts"].append(k)
                        with jax.named_scope("front1"):
                            first_front(z_at[k])
                        state["middles"].append(z_at[k])
        elif kind == "middles":
            flush_middles(what)
        elif kind == "settle":
            def store_first(normed):
                for half in range(2):
                    first[half, pl.ds(pl.multiple_of(tp * 16, 16), 16), :] = normed[16 * half : 16 * half + 16]
            with jax.named_scope("settle1"):
                own_rows = [tok[pl.ds(pl.multiple_of(tp * 16 + HALF * half, 16), 16), :] for half in range(2)]
                settle(jnp.concatenate([a.astype(F32) for a in own_rows], axis=0), store_first, 0.5, 0, None)
            spread_out(first, 0)
            spread_out(first, 1)
        else:
            with jax.named_scope("pass1"):
                pass_all(first, what)

    pair_at = pl.multiple_of(x * 128, 128)

    def mine(ref):
        both = ref[:, pl.ds(pair_at, 128)].astype(F32)
        return jnp.where(c == 0, both[:, :64], both[:, 64:])

    def rows_of(half):
        return slice(HALF * half, HALF * half + HALF)

    def project(half):
        rows = first[half]
        projected[rows_of(half), : cuts[2]] = dot_nn(rows, QA[...].reshape(D, cuts[2]))
        if cuts[2] < 384:
            projected[rows_of(half), cuts[2] : 384] = dot_nn(rows, QB[:, :, : 384 - cuts[2]].reshape(D, 384 - cuts[2]))
        ranks = dot_nt(rows, rank_down[...])
        source = dot_nn(ranks, mine(rank_up), lax.Precision.HIGHEST) + mine(bias)
        return (jnp.minimum(source, 0.0) - jnp.log1p(jnp.exp(-jnp.abs(source)))) * (1.0 / GATE_SOFTNESS)

    def attend(half, log_decay, before):
        rows = rows_of(half)
        q = projected[rows, :DK] * DK**-0.5
        k = projected[rows, DK : 2 * DK]
        v = projected[rows, 128:256]
        heads, prefix = head_out(q, k, v, log_decay)
        if before is not None:
            late = jnp.exp(-jnp.abs(before - before[HALF - 1 : HALF, :]))
            across = dot_nt(
                (q * jnp.exp(-jnp.abs(prefix))).astype(BF16), (projected[0:HALF, DK : 2 * DK] * late).astype(BF16))
            heads = heads + dot_nn(across.astype(BF16), projected[0:HALF, 128:256].astype(BF16))
        scale = lax.rsqrt(jnp.mean(heads * heads, axis=1, keepdims=True) + HEAD_FLOOR)
        gain = head_gain[:, pl.ds(pl.multiple_of(tp * DV, DV), DV)]
        mixed[rows, :] = (heads * scale * gain * silu(projected[rows, 256:384])).astype(BF16)
        return prefix

    def fronts(half, product):
        for k in range(2):
            part = product(4 * k)
            for g in range(4):
                for t in range(8):
                    sendbuf[4 * k + g, t % 2, t // 2, 16 * half : 16 * half + 16] = part[
                        t * 16 : (t + 1) * 16, g * COLS : (g + 1) * COLS].astype(BF16)
            for g in range(0, 4, 2):
                pair_copy(4 * k + g, half).start()

    def output_product(half):
        return lambda zi: dot_nt(mixed[rows_of(half), :], group_of(QB, zi, 4)[:, -128:])

    def down_product(half):
        rows, cut = rows_of(half), cuts[1]
        return lambda zi: dot_nt(hid[rows, :cut], group_of(DA, zi, 4)) + dot_nt(hid[rows, cut:], group_of(DB, zi, 4))

    def middles(half, lo, hi):
        def step(k, carry):
            middle(2 * k, half)
            return carry
        lax.fori_loop(lo, hi, step, 0)

    with jax.named_scope("gathered1a"):
        gathered(first, 0)
    with jax.named_scope("gla_a"):
        before = attend(0, project(0), None)
    with jax.named_scope("pass1b"):
        pass_all(first, 1)
    with jax.named_scope("rs2a"):
        drain_sums(None)
        fronts(0, output_product(0))
    with jax.named_scope("mid2a"):
        middles(0, 0, 4)
    with jax.named_scope("gathered1b"):
        gathered(first, 1)
    with jax.named_scope("proj_b"):
        decay_b = project(1)
    with jax.named_scope("gla_b"):
        attend(1, decay_b, before)
    with jax.named_scope("rs2b"):
        fronts(1, output_product(1))
        for half in range(2):
            drain_rows(half)
        middles(1, 0, 4)

    def put_out(half, xx, cc):
        pltpu.make_async_copy(block(third, xx, cc, half), block(out, xx, cc, half), out_sem.at[0]).start()

    def settle_second(half):
        def store(normed):
            second[half, pl.ds(pl.multiple_of(tp * 16, 16), 16), :] = normed
        settle(first[half, pl.ds(pl.multiple_of(tp * 16, 16), 16), :], store, 1.0, 1, half)
        spread_out(second, half)

    def settle_last(half):
        def store(normed):
            third[pl.ds(pl.multiple_of(tp * 16 + HALF * half, 16), 16), :] = normed
        settle(second[half, pl.ds(pl.multiple_of(tp * 16, 16), 16), :], store, 0.5, 2, half)
        spread_out(third, half)
        put_out(half, x, c)

    def mixer_front(half):
        rows = rows_of(half)
        acc[rows, : cuts[0]] = dot_nn(second[half], GA[...].reshape(D, cuts[0]))
        acc[rows, cuts[0] :] = dot_nn(second[half], GB[...].reshape(D, 1408 - cuts[0]))
        hidden(rows)

    def down_sums(half):
        fronts(half, down_product(half))
        middles(half, 0, 4)

    with jax.named_scope("settle2a"):
        settle_second(0)
    with jax.named_scope("settle2b"):
        settle_second(1)
    with jax.named_scope("pass2a"):
        pass_all(second, 0)
        gathered(second, 0)
    with jax.named_scope("gu2a"):
        mixer_front(0)
    with jax.named_scope("pass2b"):
        pass_all(second, 1)
    with jax.named_scope("rs3a"):
        drain_sums(0)
        down_sums(0)
    with jax.named_scope("gathered2b"):
        gathered(second, 1)
    with jax.named_scope("gu2b"):
        mixer_front(1)
    with jax.named_scope("rs3b"):
        drain_sums(1)
        down_sums(1)
    for half in range(2):
        drain_rows(half)
    with jax.named_scope("settle3a"):
        settle_last(0)
    with jax.named_scope("settle3b"):
        settle_last(1)
    for half in range(2):
        with jax.named_scope("pass3"):
            for s in (0, 2, 1):
                pass_on(third, s, half)
                put_out(half, from_x[s], c)
    with jax.named_scope("puts"):
        all_put()
    for half in range(2):
        with jax.named_scope("gathered3"):
            ag_copy(third, 3, half, x, other, partner).wait_recv()
            put_out(half, x, other)
            for s in (0, 2, 1):
                ag_copy(third, 4 + s, half, from_x[s], other, partner).wait_recv()
                put_out(half, from_x[s], other)
    with jax.named_scope("drain"):
        for half in range(2):
            drain_sums(half)
            drain_rows(half)
        pltpu.make_async_copy(third, out, out_sem.at[0]).wait()


def per_device(
    tokens, ffn_gate, ffn_up, ffn_down, query_proj, key_proj, value_proj, outgate_proj, output_proj,
    rank_down, rank_up, decay_bias, head_gain, norm_gain, norm_bias,
):
    operands = (
        tokens, ffn_gate, ffn_up, ffn_down.T, query_proj, key_proj, value_proj, outgate_proj, output_proj.T,
        rank_down.T, rank_up, decay_bias.reshape(1, -1), head_gain.reshape(1, -1), norm_gain, norm_bias,
    )
    items, groups, order = gather_order()
    dma = pltpu.SemaphoreType.DMA
    scratch = [pltpu.VMEM(a.shape, a.dtype) for a in operands]
    scratch += [pltpu.VMEM((NZ * NY, SHARD, tiles * LANES), BF16) for pair in WIDTHS for tiles in pair]
    scratch += [
        pltpu.VMEM((ROWS, 1408), F32),
        pltpu.VMEM((ROWS, 768), BF16),
        pltpu.VMEM((2, ROWS // 2, D), BF16),
        pltpu.VMEM((2, ROWS // 2, D), BF16),
        pltpu.VMEM((ROWS, D), BF16),
        pltpu.VMEM((ROWS, DV), BF16),
        pltpu.VMEM((ROWS, 512), F32),
        pltpu.VMEM((NZ, 2, NX, OWN, COLS), BF16),
        pltpu.VMEM((NZ, NX, OWN, COLS), BF16),
        pltpu.VMEM((NZ, NX, OWN, COLS), BF16),
        pltpu.VMEM((3, NZ, OWN, COLS), BF16),
        pltpu.VMEM((OWN, D), F32),
        dma((2 * len(WIDTHS),)), dma((len(groups),)), dma((15,)),
        dma((2,)), dma((NZ,)), dma((2, 3)), dma((2, 3)), dma((2,)), dma((7, 2)), dma((1,)),
    ]
    rows = pl.pallas_call(
        functools.partial(layer_kernel, items, groups, order),
        out_shape=jax.ShapeDtypeStruct((ROWS, D), BF16),
        in_specs=[pl.BlockSpec(memory_space=pltpu.HBM)] * 15,
        out_specs=pl.BlockSpec(memory_space=pltpu.HBM),
        scratch_shapes=scratch,
        compiler_params=pltpu.CompilerParams(
            collective_id=0, has_side_effects=True, vmem_limit_bytes=60 * 1024 * 1024),
        name="layer",
    )(*operands)
    return jnp.where(lax.axis_index("tp") >= 0, rows, jnp.zeros_like(rows))


def solution(mesh):
    finer = Mesh(
        mesh.devices.reshape(mesh.shape["rep"], NZ, NY, mesh.shape["tp"]),
        ("rep", "fs_0", "fs_1", "tp"),
    )
    return jax.shard_map(
        per_device,
        mesh=finer,
        in_specs=(
            P(REP_FS, None), P(FS, "tp"), P(FS, "tp"), P("tp", FS), P(FS, "tp"), P(FS, "tp"), P(FS, "tp"),
            P(FS, "tp"), P("tp", FS), P(), P(), P(), P(), P(), P(),
        ),
        out_specs=P(REP_FS, None),
        check_vma=False,
    )
```
